512 devices in a mesh: sp: 64 (over z, y), tp: 8 (over x, core).
Axes of the slice: x: 4, y: 8, z: 8, core: 2. Of those that a mesh axis runs over, the one named last changes fastest.
Arguments:
- tokens: bfloat16 [16384, 2048], P('sp', 'tp'), may hold values from -6 to 6
- norm_gain: float32 [2048], replicated, may hold values from 0.1 to 1.9
- query_one: bfloat16 [2048, 512], P(None, 'tp'), may hold values from -6 to 6
- key_one: bfloat16 [2048, 512], P(None, 'tp'), may hold values from -1 to 1
- query_two: bfloat16 [2048, 512], P(None, 'tp'), may hold values from -6 to 6
- key_two: bfloat16 [2048, 512], P(None, 'tp'), may hold values from -1 to 1
- value_weight: bfloat16 [2048, 1024], P(None, 'tp'), may hold values from -0.125 to 0.125
- attn_gate_weight: bfloat16 [2048, 1024], P(None, 'tp'), may hold values from -0.125 to 0.125
- conv_outer: bfloat16 [2048, 1024], P(None, 'tp'), may hold values from -0.125 to 0.125
- conv_inner: bfloat16 [2048, 1024], P(None, 'tp'), may hold values from -0.125 to 0.125
- conv_input: bfloat16 [2048, 1024], P(None, 'tp'), may hold values from -0.125 to 0.125
- conv_taps: bfloat16 [3, 1024], P(None, 'tp'), may hold values from -3.5 to 3.5
- head_lambda: float32 [8], P('tp'), may hold values from 0.3 to 0.8
- head_gain: float32 [128], replicated, may hold values from 0.1 to 1.9
- attn_out_weight: bfloat16 [1024, 2048], P('tp'), may hold values from -0.125 to 0.125
- conv_out_weight: bfloat16 [1024, 2048], P('tp'), may hold values from -0.125 to 0.125
Outputs:
- mixed: bfloat16 [16384, 2048], P(('sp', 'tp'))
The draws below stay inside these ranges and needn't reach their ends.
All inputs are finite; a program needn't handle non-finite values.
Results may differ from the reference program's by a relative error of at most 0.014.
Values may be sent and summed in bfloat16 or wider, within the bound.
A program may use at most 64 MiB of HBM per device.

```python
import math
import jax
import jax.numpy as jnp
from jax import lax

D = 2048
HEADS = 8
KEY_DIM = 64
VALUE_DIM = 128
CONV_CH = 1024
TOKENS = 16384
N_TP = 8


def draw_tokens(key, part):
    drawn = jax.random.normal(jax.random.fold_in(key, 102), (TOKENS, D), jnp.float32)
    return jnp.clip(drawn, -6.0, 6.0).astype(jnp.bfloat16)


def pair_draw(key, index):
    base = jax.random.fold_in(key, index)
    key_part, other_part = jax.random.split(base, 2)
    shape = (D, HEADS * KEY_DIM)
    factor = 1.0 / math.sqrt(D)
    key_matrix = jnp.clip(jax.random.normal(key_part, shape, jnp.float32), -6.0, 6.0) * factor
    other = jnp.clip(jax.random.normal(other_part, shape, jnp.float32), -6.0, 6.0) * factor
    return (key_matrix, other)


def query_draw(key, index):
    key_matrix, other = pair_draw(key, index)
    return jnp.clip(2.0 * other, -6.0, 6.0).astype(jnp.bfloat16)


def draw_query_one(key, part):
    return query_draw(key, 11)


def draw_key_one(key, part):
    return pair_draw(key, 11)[0].astype(jnp.bfloat16)


def draw_query_two(key, part):
    return query_draw(key, 12)


def draw_key_two(key, part):
    return pair_draw(key, 12)[0].astype(jnp.bfloat16)


def block_levels(stream_key, extent, cuts, low, high):
    factor_of = 1.0
    for axis_at, blocks in cuts:
        steps = jax.random.uniform(jax.random.fold_in(jax.random.fold_in(stream_key, 6), axis_at), (blocks,), jnp.float32, low / len(cuts), high / len(cuts))
        factor_of = factor_of * jnp.repeat(jnp.exp(steps), extent[axis_at] // blocks).reshape((-1,) + (1,) * (len(extent) - 1 - axis_at))
    return factor_of


def gaussian(own_key, shape, scale, limit, pieces=(), kind=jnp.bfloat16):
    drawn = jax.random.normal(own_key, shape, jnp.float32) * scale
    if len(pieces) > 0:
        drawn = block_levels(own_key, shape, pieces, -0.22, 0.18) * drawn
    return jnp.clip(drawn, min=-limit, max=limit).astype(kind)


def setup_inputs(seed: int = 0) -> dict:
    seeds = jax.random.split(jax.random.key(seed), 17)
    return {
        "tokens": draw_tokens(jax.random.fold_in(seeds[16], 71), 0),
        "norm_gain": jnp.clip(1.0 + 0.18 * jax.random.normal(seeds[1], (D,), jnp.float32), 0.1, 1.9),
        "query_one": draw_query_one(jax.random.fold_in(seeds[16], 71), 0),
        "key_one": draw_key_one(jax.random.fold_in(seeds[16], 71), 0),
        "query_two": draw_query_two(jax.random.fold_in(seeds[16], 71), 0),
        "key_two": draw_key_two(jax.random.fold_in(seeds[16], 71), 0),
        "value_weight": gaussian(seeds[6], (D, HEADS * VALUE_DIM), D ** -0.5, 0.125, ((1, 8),)),
        "attn_gate_weight": gaussian(seeds[7], (D, HEADS * VALUE_DIM), D ** -0.5, 0.125, ((1, 8),)),
        "conv_outer": gaussian(seeds[8], (D, CONV_CH), D ** -0.5, 0.125, ((1, 8),)),
        "conv_inner": gaussian(seeds[9], (D, CONV_CH), D ** -0.5, 0.125, ((1, 8),)),
        "conv_input": gaussian(seeds[10], (D, CONV_CH), D ** -0.5, 0.125, ((1, 8),)),
        "conv_taps": gaussian(seeds[11], (3, CONV_CH), 3 ** -0.5, 3.5, ((1, 8),)),
        "head_lambda": jnp.clip(0.3 + 0.5 * jax.random.uniform(seeds[12], (HEADS,), jnp.float32) ** block_levels(seeds[12], (HEADS,), ((0, 8),), -0.2, 0.2), 0.3, 0.8),
        "head_gain": jnp.clip(1.0 + 0.18 * jax.random.normal(seeds[13], (VALUE_DIM,), jnp.float32), 0.1, 1.9),
        "attn_out_weight": gaussian(seeds[14], (HEADS * VALUE_DIM, D), (HEADS * VALUE_DIM + CONV_CH) ** -0.5, 0.125, ((0, 8),)),
        "conv_out_weight": gaussian(seeds[15], (CONV_CH, D), (HEADS * VALUE_DIM + CONV_CH) ** -0.5, 0.125, ((0, 8),)),
    }


EPSILON = 1e-06

def one_map(queries, keys, values):
    scores = jnp.dot(queries, keys.T, preferred_element_type=jnp.float32) * (1.0 / math.sqrt(KEY_DIM))
    peak = lax.optimization_barrier(jnp.max(scores, axis=1, keepdims=True))
    weights = jnp.exp(scores - peak)
    totals = lax.optimization_barrier(jnp.sum(weights, axis=1, keepdims=True))
    return jnp.dot(weights.astype(jnp.bfloat16), values, preferred_element_type=jnp.float32) / totals

def reference(tokens, norm_gain, query_one, key_one, query_two, key_two, value_weight, attn_gate_weight, conv_outer, conv_inner, conv_input, conv_taps, head_lambda, head_gain, attn_out_weight, conv_out_weight):
    wide = tokens.astype(jnp.float32)
    inv_rms = lax.rsqrt(lax.optimization_barrier(jnp.mean(wide * wide, axis=1, keepdims=True)) + EPSILON)
    scaled = (wide * norm_gain.astype(jnp.float32)).astype(jnp.bfloat16)

    def project(matrix):
        return (jnp.dot(scaled, matrix, preferred_element_type=jnp.float32) * inv_rms).astype(jnp.bfloat16)
    first_query = project(query_one)
    first_key = project(key_one)
    second_query = project(query_two)
    second_key = project(key_two)
    values = project(value_weight)
    attn_gate = project(attn_gate_weight)
    outer = project(conv_outer)
    inner_a = project(conv_inner)
    inner_b = project(conv_input)
    block = math.gcd(TOKENS, 512)
    gain_head = head_gain.astype(jnp.float32)

    def by_head(matrix, width):
        return matrix.reshape(TOKENS, HEADS, width).transpose(1, 0, 2)

    def per_head(head_args):
        query_a, key_a, query_b, key_b, head_values, head_gate, weight_b = head_args

        def per_block(block_args):
            block_a, block_b, block_gate = block_args
            diff = one_map(block_a, key_a, head_values) - weight_b * one_map(block_b, key_b, head_values)
            normed = diff * lax.rsqrt(lax.optimization_barrier(jnp.mean(diff * diff, axis=1, keepdims=True)) + EPSILON) * gain_head
            return (normed * jax.nn.silu(block_gate.astype(jnp.float32))).astype(jnp.bfloat16)
        outputs = lax.map(per_block, (query_a.reshape(-1, block, KEY_DIM), query_b.reshape(-1, block, KEY_DIM), head_gate.reshape(-1, block, VALUE_DIM)))
        return outputs.reshape(TOKENS, VALUE_DIM)
    heads_out = lax.map(per_head, (by_head(first_query, KEY_DIM), by_head(first_key, KEY_DIM), by_head(second_query, KEY_DIM), by_head(second_key, KEY_DIM), by_head(values, VALUE_DIM), by_head(attn_gate, VALUE_DIM), head_lambda.astype(jnp.float32)))
    attn_mix = heads_out.transpose(1, 0, 2).reshape(TOKENS, HEADS * VALUE_DIM)
    product = (inner_a.astype(jnp.float32) * inner_b.astype(jnp.float32)).astype(jnp.bfloat16)
    padded = jnp.pad(product.astype(jnp.float32), ((1, 1), (0, 0)))
    taps = conv_taps.astype(jnp.float32)
    convolved = taps[0] * padded[:-2] + taps[1] * padded[1:-1] + taps[2] * padded[2:]
    conv_mix = (outer.astype(jnp.float32) * convolved).astype(jnp.bfloat16)
    head_width = HEADS // N_TP * VALUE_DIM
    conv_width = CONV_CH // N_TP
    mixed = jnp.zeros((TOKENS, D), jnp.float32)
    for group in range(N_TP):
        partial_sum = jnp.dot(attn_mix[:, group * head_width:(group + 1) * head_width], attn_out_weight[group * head_width:(group + 1) * head_width], preferred_element_type=jnp.float32)
        partial_sum = partial_sum + jnp.dot(conv_mix[:, group * conv_width:(group + 1) * conv_width], conv_out_weight[group * conv_width:(group + 1) * conv_width], preferred_element_type=jnp.float32)
        rounded = lax.optimization_barrier(partial_sum.astype(jnp.bfloat16))
        mixed = mixed + rounded.astype(jnp.float32)
    return mixed.astype(jnp.bfloat16)
```

```python
import math

import jax
import jax.numpy as jnp
from jax import lax
from jax.experimental import pallas as pl
from jax.experimental.pallas import tpu as pltpu
from jax.sharding import PartitionSpec as P

MESH = pl.DeviceIdType.MESH
EPS = 1e-06
BF = jnp.bfloat16
F32 = jnp.float32
T, FB, D, R, KD, VD = 256, 256, 2048, 8, 64, 128
NTP = 8
KEYS = R * T
HALF = D // 2
ROWS = T // NTP
QSCALE = math.log2(math.e) / math.sqrt(KD)


def dot(a, b):
    return jnp.dot(a, b, preferred_element_type=F32)


def kernel(
    tok_h, gain, wq1_h, wk1_h, wq2_h, wk2_h, wv_h, wg_h, wo_h, wi_h, wx_h, taps, lam, hgain, aw_h, cw_h,
    out,
    tok, wn, wall, acc, ss, kb, vb, qb, gate, outer, prod, edge, halo, s1, s2, osend, orecv, tsend, trecv,
    mix, wout, psend, precv,
    lsem, tok_s, tok_r, k_s, k_r, v_s, v_r, q_s, q_r, o_s, o_r, st_s, st_r, h_s, h_r, m_s, m_r, w_s, w_r, p_s, p_r,
):
    sp = lax.axis_index("sp")
    tp = lax.axis_index("tp")
    c = tp % 2
    x = tp // 2
    z = sp // 8
    y = sp % 8
    kpos = (1 - c) * z + c * y
    qpos = (1 - c) * y + c * z
    kstride = 8 - 7 * c
    qstride = 1 + 7 * c
    other = x * 2 + 1 - c

    def kdev(pos):
        return (sp + (pos - kpos) * kstride, tp)

    def qdev(pos):
        return (sp + (pos - qpos) * qstride, tp)

    def remote(src, dst, ssem, rsem, dev):
        return pltpu.make_async_remote_copy(
            src_ref=src, dst_ref=dst, send_sem=ssem, recv_sem=rsem, device_id=dev, device_id_type=MESH
        )

    prev_sp = (sp + 63) % 64
    next_sp = (sp + 1) % 64

    cp_tok = pltpu.make_async_copy(tok_h, tok.at[tp], lsem.at[0])
    cp_tok.start()
    loads = []
    for i, w in enumerate((wq1_h, wq2_h, wk1_h, wk2_h)):
        loads.append(pltpu.make_async_copy(w, wn.at[i], lsem.at[1 + i]))
    for i, w in enumerate((wv_h, wg_h, wo_h, wi_h, wx_h)):
        loads.append(pltpu.make_async_copy(w, wall.at[:, pl.ds(256 + 128 * i, 128)], lsem.at[5 + i]))
    my_half = pl.ds(pl.multiple_of(c * HALF, HALF), HALF)
    other_half = pl.ds(pl.multiple_of((1 - c) * HALF, HALF), HALF)
    loads.append(pltpu.make_async_copy(aw_h.at[:, my_half], wout.at[c, pl.ds(0, VD), :], lsem.at[10]))
    loads.append(pltpu.make_async_copy(cw_h.at[:, my_half], wout.at[c, pl.ds(VD, VD), :], lsem.at[11]))
    for cp in loads:
        cp.start()

    barrier = pltpu.get_barrier_semaphore()

    def greet(dev):
        pl.semaphore_signal(barrier, inc=1, device_id=dev, device_id_type=MESH)

    for d in range(1, 8):
        greet((sp, (tp + d) % 8))
        greet(kdev((kpos + d) % 8))
        greet(qdev((qpos + d) % 8))
    greet((prev_sp, tp))
    greet((next_sp, tp))
    pl.semaphore_wait(barrier, 23)

    cp_tok.wait()

    def tok_to(j):
        return remote(tok.at[tp], tok.at[tp], tok_s.at[j], tok_r.at[tp], (sp, ((x + j) % 4) * 2 + c))

    def tok_fwd(t, slot):
        return remote(tok.at[t], tok.at[t], tok_s.at[slot], tok_r.at[t], (sp, other))

    tok_to(2).start()
    tok_to(1).start()
    tok_to(3).start()
    tok_fwd(tp, 0).start()

    wcopies = [
        remote(aw_h.at[:, other_half], wout.at[c, pl.ds(0, VD), :], w_s.at[0], w_r.at[0], (sp, other)),
        remote(cw_h.at[:, other_half], wout.at[c, pl.ds(VD, VD), :], w_s.at[1], w_r.at[1], (sp, other)),
    ]
    for cp in wcopies:
        cp.start()

    for cp in loads[:4]:
        cp.wait()

    def join(i, carry):
        rows = pl.ds(pl.multiple_of(i * 256, 256), 256)
        wall[rows, pl.ds(0, 128)] = jnp.concatenate([wn[0, rows, :], wn[1, rows, :]], axis=1)
        wall[rows, pl.ds(128, 128)] = jnp.concatenate([wn[2, rows, :], wn[3, rows, :]], axis=1)
        return carry

    lax.fori_loop(0, 8, join, 0)
    for cp in loads[4:9]:
        cp.wait()

    acc[...] = jnp.zeros_like(acc)
    ss[...] = jnp.zeros_like(ss)

    def project(step, carry):
        j = step // 2
        odd = step % 2
        dx = jnp.where(j == 0, 0, jnp.where(j == 1, 3, jnp.where(j == 2, 1, 2)))
        chip = (x + dx) % 4
        cc = (1 - odd) * c + odd * (1 - c)
        t = chip * 2 + cc

        @pl.when(step > 0)
        def _():
            remote(tok.at[t], tok.at[t], tok_s.at[0], tok_r.at[t], (sp, other)).wait_recv()

        @pl.when((step > 1) & (odd == 0))
        def _():
            tok_fwd(t, 3 + j).start()

        block = tok[t].astype(F32)
        sq = block * block
        ss[...] += sq[:, :128] + sq[:, 128:]
        g = gain[:, pl.ds(pl.multiple_of(t * FB, FB), FB)]
        scaled = (block * g).astype(BF)
        acc[...] += dot(scaled, wall[pl.ds(pl.multiple_of(t * FB, FB), FB), :])
        return carry

    lax.fori_loop(0, 8, project, 0)

    inv = lax.rsqrt(jnp.sum(ss[...], axis=1, keepdims=True) / D + EPS)

    kb[kpos] = (acc[:, 128:256] * inv).astype(BF)
    vb[kpos] = (acc[:, 256:384] * inv).T.astype(BF)
    qb[qpos] = (acc[:, 0:128] * (inv * QSCALE)).T.astype(BF)

    def k_to(d):
        return remote(kb.at[kpos], kb.at[kpos], k_s.at[d], k_r.at[kpos], kdev((kpos + d) % 8))

    def v_to(d):
        return remote(vb.at[kpos], vb.at[kpos], v_s.at[d], v_r.at[kpos], kdev((kpos + d) % 8))

    def q_to(d):
        return remote(qb.at[qpos], qb.at[qpos], q_s.at[d], q_r.at[qpos], qdev((qpos + d) % 8))

    order = (4, 3, 5, 2, 6, 1, 7)
    for d in order:
        k_to(d).start()
    for d in order:
        v_to(d).start()
    for d in order:
        q_to(d).start()

    gate[...] = (acc[:, 384:512] * inv).astype(BF)
    outer[...] = (acc[:, 512:640] * inv).astype(BF)
    pr = ((acc[:, 640:768] * inv).astype(BF).astype(F32) * (acc[:, 768:896] * inv).astype(BF).astype(F32)).astype(BF)
    pr = pr.astype(F32)
    prod[...] = pr
    edge[0] = pr[0:8]
    edge[1] = pr[T - 8 : T]
    to_prev = remote(edge.at[0], halo.at[1], h_s.at[0], h_r.at[1], (prev_sp, tp))
    to_next = remote(edge.at[1], halo.at[0], h_s.at[1], h_r.at[0], (next_sp, tp))
    to_prev.start()
    to_next.start()
    to_prev.wait_recv()
    to_next.wait_recv()
    before = jnp.where(sp == 0, 0.0, halo[0][7:8, :])
    after = jnp.where(sp == 63, 0.0, halo[1][0:1, :])
    cur = prod[...]
    rows = lax.broadcasted_iota(jnp.int32, (T, VD), 0)
    up = jnp.where(rows == 0, before, pltpu.roll(cur, 1, 0))
    down = jnp.where(rows == T - 1, after, pltpu.roll(cur, T - 1, 0))
    tp32 = taps[...].astype(F32)
    conv = tp32[0:1] * up + tp32[1:2] * cur + tp32[2:3] * down
    mix[c, :, pl.ds(VD, VD)] = (outer[...].astype(F32) * conv).astype(BF)

    def kv_wait(d, carry):
        pos = (kpos + d) % 8
        remote(kb.at[pos], kb.at[pos], k_s.at[0], k_r.at[pos], kdev(pos)).wait_recv()
        remote(vb.at[pos], vb.at[pos], v_s.at[0], v_r.at[pos], kdev(pos)).wait_recv()
        return carry

    lax.fori_loop(1, 8, kv_wait, 0)

    zero = jnp.zeros((KD, T), BF)

    def scores(qm, n, s_ref, peak):
        s = dot(kb[n], qm)
        s_ref[pl.ds(n * T, T), :] = s
        top = jnp.max(s.reshape(T // 8, 8, T), axis=0)
        return top if peak is None else jnp.maximum(peak, top)

    def apply(n, s_ref, peak, state):
        p = jnp.exp2(s_ref[pl.ds(n * T, T), :] - peak)
        part = jnp.sum(p.reshape(T // 8, 8, T), axis=0)
        o = dot(vb[n], p.astype(BF))
        return (part, o) if state is None else (state[0] + part, state[1] + o)

    def one_block(i, carry):
        odd = i % 2
        mag = 4 - (i + 1) // 2
        off = odd * mag + (1 - odd) * ((8 - mag) % 8)
        pos = (qpos + off) % 8

        @pl.when(i < 7)
        def _():
            remote(qb.at[pos], qb.at[pos], q_s.at[0], q_r.at[pos], qdev(pos)).wait_recv()

        q = qb[pos]
        q1 = jnp.concatenate([q[:KD], zero], axis=0)
        q2 = jnp.concatenate([zero, q[KD:]], axis=0)
        peak = None
        for n in range(R):
            peak = scores(q1, n, s1, peak)
        peak1 = jnp.max(peak, axis=0, keepdims=True)
        peak = None
        state = None
        for n in range(R):
            peak = scores(q2, n, s2, peak)
            state = apply(n, s1, peak1, state)
        peak2 = jnp.max(peak, axis=0, keepdims=True)
        sum1 = jnp.sum(state[0], axis=0, keepdims=True)
        osend[pos, pl.ds(0, VD), :] = state[1].astype(BF)
        state = None
        for n in range(R):
            state = apply(n, s2, peak2, state)
        sum2 = jnp.sum(state[0], axis=0, keepdims=True)
        osend[pos, pl.ds(VD, VD), :] = state[1].astype(BF)
        tsend[pos] = jnp.concatenate([peak1, sum1, peak2, sum2, peak1, sum1, peak2, sum2], axis=0)

        @pl.when(i < 7)
        def _():
            remote(osend.at[pos], orecv.at[qpos], o_s.at[pos], o_r.at[qpos], qdev(pos)).start()
            remote(tsend.at[pos], trecv.at[qpos], st_s.at[pos], st_r.at[qpos], qdev(pos)).start()

        return carry

    lax.fori_loop(0, 8, one_block, 0)

    orecv[qpos] = osend[qpos]
    trecv[qpos] = tsend[qpos]

    def o_wait(d, carry):
        pos = (qpos + d) % 8
        remote(osend.at[pos], orecv.at[pos], o_s.at[pos], o_r.at[pos], qdev(pos)).wait_recv()
        remote(tsend.at[pos], trecv.at[pos], st_s.at[pos], st_r.at[pos], qdev(pos)).wait_recv()
        return carry

    lax.fori_loop(1, 8, o_wait, 0)

    def merged(row, at):
        peak = trecv[0, pl.ds(row, 1), :]
        for n in range(1, R):
            peak = jnp.maximum(peak, trecv[n, pl.ds(row, 1), :])
        total = None
        for n in range(R):
            w = jnp.exp2(trecv[n, pl.ds(row, 1), :] - peak)
            part = w * trecv[n, pl.ds(row + 1, 1), :]
            o = w * orecv[n, pl.ds(at, VD), :].astype(F32)
            total = (part, o) if total is None else (total[0] + part, total[1] + o)
        return total[1] / total[0]

    diff = merged(0, 0) - lam[0] * merged(2, VD)
    diff = (diff * lax.rsqrt(jnp.mean(diff * diff, axis=0, keepdims=True) + EPS)).T
    g32 = gate[...].astype(F32)
    mix[c, :, pl.ds(0, VD)] = (diff * hgain[...] * (g32 / (1.0 + jnp.exp(-g32)))).astype(BF)

    share = remote(mix.at[c], mix.at[c], m_s, m_r, (sp, other))
    share.start()
    for cp in loads[9:]:
        cp.wait()
    for i in range(2):
        wcopies[i].wait_recv()
    share.wait_recv()

    def p_copy(chip, core):
        return remote(
            psend.at[chip, pl.ds(pl.multiple_of(core * ROWS, ROWS), ROWS), :],
            precv.at[tp],
            p_s.at[chip * 2 + core],
            p_r.at[tp],
            (sp, chip * 2 + core),
        )

    def to_chip(i, carry):
        chip = (x + jnp.where(i == 0, 2, jnp.where(i == 1, 1, jnp.where(i == 2, 3, 0)))) % 4
        rows = pl.ds(pl.multiple_of(chip * 2 * ROWS, 2 * ROWS), 2 * ROWS)
        psend[chip] = (dot(mix[0, rows, :], wout[0]) + dot(mix[1, rows, :], wout[1])).astype(BF)

        @pl.when(i < 3)
        def _():
            p_copy(chip, c).start()

        p_copy(chip, 1 - c).start()
        return carry

    lax.fori_loop(0, 4, to_chip, 0)
    precv[tp] = psend[x, pl.ds(pl.multiple_of(c * ROWS, ROWS), ROWS), :]

    def p_wait(d, carry):
        src = (tp + d) % 8
        remote(
            psend.at[0, pl.ds(0, ROWS), :], precv.at[src], p_s.at[0], p_r.at[src], (sp, src)
        ).wait_recv()
        return carry

    lax.fori_loop(1, 8, p_wait, 0)
    for half in range(2):
        total = precv[half].astype(F32)
        for n in range(1, 4):
            total += precv[2 * n + half].astype(F32)
        out[:, pl.ds(half * HALF, HALF)] = total.astype(BF)

    tok_fwd(tp, 0).wait_send()
    for j in (1, 2, 3):
        tok_to(j).wait_send()
        tok_fwd(tp, 3 + j).wait_send()
    for d in range(1, 8):
        k_to(d).wait_send()
        v_to(d).wait_send()
        q_to(d).wait_send()
        pos = (qpos + d) % 8
        remote(osend.at[pos], orecv.at[qpos], o_s.at[pos], o_r.at[qpos], qdev(pos)).wait_send()
        remote(tsend.at[pos], trecv.at[qpos], st_s.at[pos], st_r.at[qpos], qdev(pos)).wait_send()
        dst = (tp + d) % 8
        p_copy(dst // 2, dst % 2).wait_send()
    to_prev.wait_send()
    to_next.wait_send()
    share.wait_send()
    for cp in wcopies:
        cp.wait_send()


def local(tokens, norm_gain, q1, k1, q2, k2, wv, wg, wo, wi, wx, taps, lam, hgain, aw, cw):
    hbm = pl.BlockSpec(memory_space=pl.ANY)
    vm = pl.BlockSpec(memory_space=pltpu.VMEM)
    sm = pl.BlockSpec(memory_space=pltpu.SMEM)
    dma = pltpu.SemaphoreType.DMA
    v = pltpu.VMEM
    return pl.pallas_call(
        kernel,
        out_shape=jax.ShapeDtypeStruct((ROWS, D), BF),
        in_specs=[hbm, vm] + [hbm] * 9 + [vm, sm, vm, hbm, hbm],
        out_specs=vm,
        scratch_shapes=[
            v((8, T, FB), BF), v((4, D, KD), BF), v((D, 896), BF), v((T, 896), F32), v((T, 128), F32),
            v((R, T, 128), BF), v((R, VD, T), BF), v((R, 128, T), BF),
            v((T, VD), BF), v((T, VD), BF), v((T, VD), F32), v((2, 8, VD), F32), v((2, 8, VD), F32),
            v((KEYS, T), F32), v((KEYS, T), F32),
            v((R, 2 * VD, T), BF), v((R, 2 * VD, T), BF), v((R, 8, T), F32), v((R, 8, T), F32),
            v((2, T, 2 * VD), BF), v((2, 2 * VD, HALF), BF), v((4, 2 * ROWS, HALF), BF), v((8, ROWS, HALF), BF),
            dma((12,)), dma((8,)), dma((8,)), dma((8,)), dma((8,)), dma((8,)), dma((8,)), dma((8,)), dma((8,)),
            dma((8,)), dma((8,)), dma((8,)), dma((8,)), dma((2,)), dma((2,)), dma, dma, dma((2,)), dma((2,)),
            dma((8,)), dma((8,)),
        ],
        compiler_params=pltpu.CompilerParams(
            collective_id=0, has_side_effects=True, vmem_limit_bytes=48 * 1024 * 1024
        ),
        name="layer",
    )(tokens, norm_gain.reshape(1, D), q1, k1, q2, k2, wv, wg, wo, wi, wx, taps, lam, hgain.reshape(1, VD), aw, cw)


def solution(mesh):
    col = P(None, "tp")
    return jax.shard_map(
        local,
        mesh=mesh,
        in_specs=(P("sp", "tp"), P()) + (col,) * 10 + (P("tp"), P(), P("tp", None), P("tp", None)),
        out_specs=P(("sp", "tp"), None),
        check_vma=False,
    )
```

```python
import math

import jax
import jax.numpy as jnp
from jax import lax
from jax.experimental import pallas as pl
from jax.experimental.pallas import tpu as pltpu
from jax.sharding import PartitionSpec as P

MESH = pl.DeviceIdType.MESH
EPS = 1e-06
BF = jnp.bfloat16
F32 = jnp.float32
T, FB, D, R, KD, VD = 256, 256, 2048, 8, 64, 128
NTP = 8
KEYS = R * T
HALF = D // 2
ROWS = T // NTP
QSCALE = math.log2(math.e) / math.sqrt(KD)


def dot(a, b):
    return jnp.dot(a, b, preferred_element_type=F32)


def kernel(
    tok_h, gain, wq1_h, wk1_h, wq2_h, wk2_h, wv_h, wg_h, wo_h, wi_h, wx_h, taps, lam, hgain, aw_h, cw_h,
    out,
    tok, wn, wall, acc, ss, kb, vb, qb, gate, outer, prod, edge, halo, s1, s2, osend, orecv, tsend, trecv,
    mix, wout, psend, precv,
    lsem, tok_s, tok_r, k_s, k_r, v_s, v_r, q_s, q_r, o_s, o_r, st_s, st_r, h_s, h_r, m_s, m_r, w_s, w_r, p_s, p_r,
):
    sp = lax.axis_index("sp")
    tp = lax.axis_index("tp")
    c = tp % 2
    x = tp // 2
    z = sp // 8
    y = sp % 8
    kpos = (1 - c) * z + c * y
    qpos = (1 - c) * y + c * z
    kstride = 8 - 7 * c
    qstride = 1 + 7 * c
    other = x * 2 + 1 - c

    def kdev(pos):
        return (sp + (pos - kpos) * kstride, tp)

    def qdev(pos):
        return (sp + (pos - qpos) * qstride, tp)

    def remote(src, dst, ssem, rsem, dev):
        return pltpu.make_async_remote_copy(
            src_ref=src, dst_ref=dst, send_sem=ssem, recv_sem=rsem, device_id=dev, device_id_type=MESH
        )

    prev_sp = (sp + 63) % 64
    next_sp = (sp + 1) % 64

    cp_tok = pltpu.make_async_copy(tok_h, tok.at[tp], lsem.at[0])
    cp_tok.start()
    loads = []
    for i, w in enumerate((wq1_h, wq2_h, wk1_h, wk2_h)):
        loads.append(pltpu.make_async_copy(w, wn.at[pl.ds(KD * i, KD), :], lsem.at[1 + i]))
    for i, w in enumerate((wv_h, wg_h, wo_h, wi_h, wx_h)):
        loads.append(pltpu.make_async_copy(w, wall.at[:, pl.ds(128 * i, 128)], lsem.at[5 + i]))
    my_half = pl.ds(pl.multiple_of(c * HALF, HALF), HALF)
    other_half = pl.ds(pl.multiple_of((1 - c) * HALF, HALF), HALF)
    loads.append(pltpu.make_async_copy(aw_h.at[:, my_half], wout.at[c, pl.ds(0, VD), :], lsem.at[10]))
    loads.append(pltpu.make_async_copy(cw_h.at[:, my_half], wout.at[c, pl.ds(VD, VD), :], lsem.at[11]))
    for cp in loads:
        cp.start()

    barrier = pltpu.get_barrier_semaphore()

    def greet(dev):
        pl.semaphore_signal(barrier, inc=1, device_id=dev, device_id_type=MESH)

    right_chip = (sp, ((x + 1) % 4) * 2 + c)
    left_chip = (sp, ((x + 3) % 4) * 2 + c)
    partner = (sp, other)
    k_right, k_left = kdev((kpos + 1) % 8), kdev((kpos + 7) % 8)
    q_right, q_left = qdev((qpos + 1) % 8), qdev((qpos + 7) % 8)
    greeted = (right_chip, left_chip, partner, k_right, k_left, q_right, q_left, (prev_sp, tp), (next_sp, tp))
    for dev in greeted:
        greet(dev)
    pl.semaphore_wait(barrier, len(greeted))

    pending = []

    def send(src, dst, ssem, rsem, dev):
        cp = remote(src, dst, ssem, rsem, dev)
        cp.start()
        pending.append(cp)

    def arrived(ref, rsem):
        remote(ref, ref, rsem, rsem, partner).wait_recv()

    top, bottom = pl.ds(0, T // 2), pl.ds(T // 2, T // 2)
    halves = (top, bottom)

    def tok_send(t, half, slot, dev):
        ref = tok.at[t, halves[half], :]
        send(ref, ref, tok_s.at[slot], tok_r.at[t, half], dev)

    def tok_wait(t, half):
        arrived(tok.at[t, halves[half], :], tok_r.at[t, half])

    cp_tok.wait()
    tok_send(tp, 0, 0, right_chip)
    tok_send(tp, 1, 1, left_chip)
    tok_send(tp, 1, 2, right_chip)
    tok_send(tp, 0, 3, left_chip)
    tok_send(tp, 0, 4, partner)
    tok_send(tp, 1, 5, partner)

    for cp in loads[:9]:
        cp.wait()

    def project(t, first=False):
        block = tok[t].astype(F32)
        sq = block * block
        sq = sq[:, :128] + sq[:, 128:]
        at = pl.ds(pl.multiple_of(t * FB, FB), FB)
        scaled = (block * gain[:, at]).astype(BF)
        narrow = lax.dot_general(scaled, wn[:, at], (((1,), (1,)), ((), ())), preferred_element_type=F32)
        wide = dot(scaled, wall[at, :])
        if first:
            ss[...] = sq
            acc[:, pl.ds(0, 256)] = narrow
            acc[:, pl.ds(256, 640)] = wide
        else:
            ss[...] += sq
            acc[:, pl.ds(0, 256)] += narrow
            acc[:, pl.ds(256, 640)] += wide

    xl, xr, xo = (x + 3) % 4, (x + 1) % 4, (x + 2) % 4
    d = 1 - c
    project(tp, True)
    tok_wait(other, 0)
    tok_wait(other, 1)
    project(other)
    tok_wait(xl * 2 + c, 0)
    tok_send(xl * 2 + c, 0, 6, right_chip)
    tok_send(xl * 2 + c, 0, 7, partner)
    tok_wait(xr * 2 + c, 1)
    tok_send(xr * 2 + c, 1, 8, left_chip)
    tok_send(xr * 2 + c, 1, 9, partner)
    tok_wait(xl * 2 + c, 1)
    tok_send(xl * 2 + c, 1, 10, partner)
    tok_wait(xr * 2 + c, 0)
    tok_send(xr * 2 + c, 0, 11, partner)
    project(xl * 2 + c)
    project(xr * 2 + c)
    tok_wait(xl * 2 + d, 0)
    tok_wait(xl * 2 + d, 1)
    project(xl * 2 + d)
    tok_wait(xr * 2 + d, 0)
    tok_wait(xr * 2 + d, 1)
    project(xr * 2 + d)
    tok_wait(xo * 2 + c, 0)
    tok_send(xo * 2 + c, 0, 12, partner)
    tok_wait(xo * 2 + c, 1)
    tok_send(xo * 2 + c, 1, 13, partner)
    project(xo * 2 + c)
    tok_wait(xo * 2 + d, 0)
    tok_wait(xo * 2 + d, 1)
    project(xo * 2 + d)

    inv = lax.rsqrt(jnp.sum(ss[...], axis=1, keepdims=True) / D + EPS)

    def k_send(pos, slot, dev):
        send(kb.at[pos], kb.at[pos], k_s.at[slot], k_r.at[pos], dev)

    def v_send(pos, slot, dev):
        send(vb.at[pos], vb.at[pos], v_s.at[slot], v_r.at[pos], dev)

    def q_send(pos, slot, dev):
        send(qb.at[pos], qb.at[pos], q_s.at[slot], q_r.at[pos], dev)

    def q_part(pos, part, slot, dev):
        ref = qb.at[pos, pl.ds(KD * part, KD), :]
        send(ref, ref, q_s.at[slot], q_r.at[pos if part == 0 else 8], dev)

    kb[kpos] = (acc[:, 128:256] * inv).astype(BF)
    k_send(kpos, 0, k_right)
    k_send(kpos, 1, k_left)
    vb[kpos] = (acc[:, 256:384] * inv).T.astype(BF)
    v_send(kpos, 0, k_left)
    v_send(kpos, 1, k_right)
    qb[qpos] = (acc[:, 0:128] * (inv * QSCALE)).T.astype(BF)
    q_send(qpos, 0, q_right)
    q_send(qpos, 1, q_left)

    def ring_step(n):
        kl, kr, ql, qr = (kpos + 8 - n) % 8, (kpos + n) % 8, (qpos + 8 - n) % 8, (qpos + n) % 8
        arrived(kb.at[kl], k_r.at[kl])
        if n < 4:
            k_send(kl, 2 * n, k_right)
            arrived(kb.at[kr], k_r.at[kr])
            if n < 3:
                k_send(kr, 2 * n + 1, k_left)
        arrived(vb.at[kr], v_r.at[kr])
        if n < 4:
            v_send(kr, 2 * n, k_left)
            arrived(vb.at[kl], v_r.at[kl])
            if n < 3:
                v_send(kl, 2 * n + 1, k_right)
        if n < 4:
            arrived(qb.at[ql], q_r.at[ql])
            if n < 3:
                q_send(ql, 2 * n, q_right)
            else:
                q_part(ql, 0, 6, q_right)
            arrived(qb.at[qr], q_r.at[qr])
            if n < 3:
                q_send(qr, 2 * n + 1, q_left)
            else:
                q_part(qr, 1, 7, q_left)
        else:
            arrived(qb.at[ql, pl.ds(0, KD), :], q_r.at[ql])
            arrived(qb.at[ql, pl.ds(KD, KD), :], q_r.at[8])

    gate[...] = (acc[:, 384:512] * inv).astype(BF)
    outer[...] = (acc[:, 512:640] * inv).astype(BF)
    pr = ((acc[:, 640:768] * inv).astype(BF).astype(F32) * (acc[:, 768:896] * inv).astype(BF).astype(F32)).astype(BF)
    pr = pr.astype(F32)
    prod[...] = pr
    edge[0] = pr[0:8]
    edge[1] = pr[T - 8 : T]
    to_prev = remote(edge.at[0], halo.at[1], h_s.at[0], h_r.at[1], (prev_sp, tp))
    to_next = remote(edge.at[1], halo.at[0], h_s.at[1], h_r.at[0], (next_sp, tp))
    to_prev.start()
    to_next.start()
    ring_step(1)
    to_prev.wait_recv()
    to_next.wait_recv()
    before = jnp.where(sp == 0, 0.0, halo[0][7:8, :])
    after = jnp.where(sp == 63, 0.0, halo[1][0:1, :])
    cur = prod[...]
    rows = lax.broadcasted_iota(jnp.int32, (T, VD), 0)
    up = jnp.where(rows == 0, before, pltpu.roll(cur, 1, 0))
    down = jnp.where(rows == T - 1, after, pltpu.roll(cur, T - 1, 0))
    tp32 = taps[...].astype(F32)
    conv = tp32[0:1] * up + tp32[1:2] * cur + tp32[2:3] * down
    mix[c, :, pl.ds(VD, VD)] = (outer[...].astype(F32) * conv).astype(BF)

    for n in (2, 3, 4):
        ring_step(n)

    send(aw_h.at[:, other_half], wout.at[c, pl.ds(0, VD), :], w_s.at[0], w_r.at[0], partner)
    send(cw_h.at[:, other_half], wout.at[c, pl.ds(VD, VD), :], w_s.at[1], w_r.at[1], partner)

    zero = jnp.zeros((KD, T), BF)

    def scores(qm, n, s_ref, peak):
        s = dot(kb[n], qm)
        s_ref[pl.ds(n * T, T), :] = s
        top = jnp.max(s.reshape(T // 8, 8, T), axis=0)
        return top if peak is None else jnp.maximum(peak, top)

    def apply(n, s_ref, peak, state):
        p = jnp.exp2(s_ref[pl.ds(n * T, T), :] - peak)
        part = jnp.sum(p.reshape(T // 8, 8, T), axis=0)
        o = dot(vb[n], p.astype(BF))
        return (part, o) if state is None else (state[0] + part, state[1] + o)

    def one_block(i, carry):
        odd = i % 2
        mag = 4 - (i + 1) // 2
        off = odd * mag + (1 - odd) * ((8 - mag) % 8)
        pos = (qpos + off) % 8

        q = qb[pos]
        q1 = jnp.concatenate([q[:KD], zero], axis=0)
        q2 = jnp.concatenate([zero, q[KD:]], axis=0)
        peak = None
        for n in range(R):
            peak = scores(q1, n, s1, peak)
        peak1 = jnp.max(peak, axis=0, keepdims=True)
        peak = None
        state = None
        for n in range(R):
            peak = scores(q2, n, s2, peak)
            state = apply(n, s1, peak1, state)
        peak2 = jnp.max(peak, axis=0, keepdims=True)
        sum1 = jnp.sum(state[0], axis=0, keepdims=True)
        osend[pos, pl.ds(0, VD), :] = state[1].astype(BF)
        state = None
        for n in range(R):
            state = apply(n, s2, peak2, state)
        sum2 = jnp.sum(state[0], axis=0, keepdims=True)
        osend[pos, pl.ds(VD, VD), :] = state[1].astype(BF)
        tsend[pos] = jnp.concatenate([peak1, sum1, peak2, sum2, peak1, sum1, peak2, sum2], axis=0)

        @pl.when(i < 7)
        def _():
            remote(osend.at[pos], orecv.at[qpos], o_s.at[pos], o_r.at[qpos], qdev(pos)).start()
            remote(tsend.at[pos], trecv.at[qpos], st_s.at[pos], st_r.at[qpos], qdev(pos)).start()

        return carry

    lax.fori_loop(0, 8, one_block, 0)

    orecv[qpos] = osend[qpos]
    trecv[qpos] = tsend[qpos]

    def o_wait(d, carry):
        pos = (qpos + d) % 8
        remote(osend.at[pos], orecv.at[pos], o_s.at[pos], o_r.at[pos], qdev(pos)).wait_recv()
        remote(tsend.at[pos], trecv.at[pos], st_s.at[pos], st_r.at[pos], qdev(pos)).wait_recv()
        return carry

    lax.fori_loop(1, 8, o_wait, 0)

    def merged(row, at):
        peak = trecv[0, pl.ds(row, 1), :]
        for n in range(1, R):
            peak = jnp.maximum(peak, trecv[n, pl.ds(row, 1), :])
        total = None
        for n in range(R):
            w = jnp.exp2(trecv[n, pl.ds(row, 1), :] - peak)
            part = w * trecv[n, pl.ds(row + 1, 1), :]
            o = w * orecv[n, pl.ds(at, VD), :].astype(F32)
            total = (part, o) if total is None else (total[0] + part, total[1] + o)
        return total[1] / total[0]

    diff = merged(0, 0) - lam[0] * merged(2, VD)
    diff = (diff * lax.rsqrt(jnp.mean(diff * diff, axis=0, keepdims=True) + EPS)).T
    g32 = gate[...].astype(F32)
    mix[c, :, pl.ds(0, VD)] = (diff * hgain[...] * (g32 / (1.0 + jnp.exp(-g32)))).astype(BF)

    share = remote(mix.at[c], mix.at[c], m_s, m_r, (sp, other))
    share.start()
    for cp in loads[9:]:
        cp.wait()
    arrived(wout.at[1 - c, pl.ds(0, VD), :], w_r.at[0])
    arrived(wout.at[1 - c, pl.ds(VD, VD), :], w_r.at[1])
    share.wait_recv()

    def p_copy(chip, core):
        return remote(
            psend.at[chip, pl.ds(pl.multiple_of(core * ROWS, ROWS), ROWS), :],
            precv.at[tp],
            p_s.at[chip * 2 + core],
            p_r.at[tp],
            (sp, chip * 2 + core),
        )

    def to_chip(i, carry):
        chip = (x + jnp.where(i == 0, 2, jnp.where(i == 1, 1, jnp.where(i == 2, 3, 0)))) % 4
        rows = pl.ds(pl.multiple_of(chip * 2 * ROWS, 2 * ROWS), 2 * ROWS)
        psend[chip] = (dot(mix[0, rows, :], wout[0]) + dot(mix[1, rows, :], wout[1])).astype(BF)

        @pl.when(i < 3)
        def _():
            p_copy(chip, c).start()

        p_copy(chip, 1 - c).start()
        return carry

    lax.fori_loop(0, 4, to_chip, 0)
    precv[tp] = psend[x, pl.ds(pl.multiple_of(c * ROWS, ROWS), ROWS), :]

    def p_wait(d, carry):
        src = (tp + d) % 8
        remote(
            psend.at[0, pl.ds(0, ROWS), :], precv.at[src], p_s.at[0], p_r.at[src], (sp, src)
        ).wait_recv()
        return carry

    lax.fori_loop(1, 8, p_wait, 0)
    for half in range(2):
        total = precv[half].astype(F32)
        for n in range(1, 4):
            total += precv[2 * n + half].astype(F32)
        out[:, pl.ds(half * HALF, HALF)] = total.astype(BF)

    for cp in pending:
        cp.wait_send()
    for d in range(1, 8):
        pos = (qpos + d) % 8
        remote(osend.at[pos], orecv.at[qpos], o_s.at[pos], o_r.at[qpos], qdev(pos)).wait_send()
        remote(tsend.at[pos], trecv.at[qpos], st_s.at[pos], st_r.at[qpos], qdev(pos)).wait_send()
        dst = (tp + d) % 8
        p_copy(dst // 2, dst % 2).wait_send()
    to_prev.wait_send()
    to_next.wait_send()
    share.wait_send()


def local(tokens, norm_gain, q1, k1, q2, k2, wv, wg, wo, wi, wx, taps, lam, hgain, aw, cw):
    hbm = pl.BlockSpec(memory_space=pltpu.HBM)
    vm = pl.BlockSpec(memory_space=pltpu.VMEM)
    sm = pl.BlockSpec(memory_space=pltpu.SMEM)
    dma = pltpu.SemaphoreType.DMA
    v = pltpu.VMEM
    return pl.pallas_call(
        kernel,
        out_shape=jax.ShapeDtypeStruct((ROWS, D), BF),
        in_specs=[hbm, vm] + [hbm] * 9 + [vm, sm, vm, hbm, hbm],
        out_specs=vm,
        scratch_shapes=[
            v((8, T, FB), BF), v((4 * KD, D), BF), v((D, 640), BF), v((T, 896), F32), v((T, 128), F32),
            v((R, T, 128), BF), v((R, VD, T), BF), v((R, 128, T), BF),
            v((T, VD), BF), v((T, VD), BF), v((T, VD), F32), v((2, 8, VD), F32), v((2, 8, VD), F32),
            v((KEYS, T), F32), v((KEYS, T), F32),
            v((R, 2 * VD, T), BF), v((R, 2 * VD, T), BF), v((R, 8, T), F32), v((R, 8, T), F32),
            v((2, T, 2 * VD), BF), v((2, 2 * VD, HALF), BF), v((4, 2 * ROWS, HALF), BF), v((8, ROWS, HALF), BF),
            dma((12,)), dma((14,)), dma((8, 2)), dma((8,)), dma((8,)), dma((8,)), dma((8,)), dma((8,)), dma((9,)),
            dma((8,)), dma((8,)), dma((8,)), dma((8,)), dma((2,)), dma((2,)), dma, dma, dma((2,)), dma((2,)),
            dma((8,)), dma((8,)),
        ],
        compiler_params=pltpu.CompilerParams(
            collective_id=0, has_side_effects=True, vmem_limit_bytes=67043328
        ),
        name="layer",
    )(tokens, norm_gain.reshape(1, D), q1.T, k1.T, q2.T, k2.T, wv, wg, wo, wi, wx, taps, lam, hgain.reshape(1, VD), aw, cw)


def solution(mesh):
    col = P(None, "tp")
    return jax.shard_map(
        local,
        mesh=mesh,
        in_specs=(P("sp", "tp"), P()) + (col,) * 10 + (P("tp"), P(), P("tp", None), P("tp", None)),
        out_specs=P(("sp", "tp"), None),
        check_vma=False,
    )
```

```python
import math

import jax
import jax.numpy as jnp
from jax import lax
from jax.experimental import pallas as pl
from jax.experimental.pallas import tpu as pltpu
from jax.sharding import PartitionSpec as P

MESH = pl.DeviceIdType.MESH
EPS = 1e-06
BF = jnp.bfloat16
F32 = jnp.float32
T, FB, D, R, KD, VD = 256, 256, 2048, 8, 64, 128
NTP = 8
KEYS = R * T
HALF = D // 2
ROWS = T // NTP
QSCALE = math.log2(math.e) / math.sqrt(KD)


def dot(a, b):
    return jnp.dot(a, b, preferred_element_type=F32)


def kernel(
    tok_h, gain, wq1_h, wk1_h, wq2_h, wk2_h, wv_h, wg_h, wo_h, wi_h, wx_h, taps, lam, hgain, aw_h, cw_h,
    out,
    tok, wn, wall, acc, ss, kb, vb, qb, gate, outer, prod, edge, halo, s1, s2, osend, orecv, tsend, trecv,
    mix, wout, psend, precv, wa, csum, amix, arecv,
    lsem, tok_s, tok_r, k_s, k_r, v_s, v_r, q_s, q_r, o_s, o_r, st_s, st_r, h_s, h_r, m_s, m_r, w_s, w_r, p_s, p_r, wa_s, wa_r, a_s, a_r,
):
    sp = lax.axis_index("sp")
    tp = lax.axis_index("tp")
    c = tp % 2
    x = tp // 2
    z = sp // 8
    y = sp % 8
    kpos = (1 - c) * z + c * y
    qpos = (1 - c) * y + c * z
    kstride = 8 - 7 * c
    qstride = 1 + 7 * c
    other = x * 2 + 1 - c

    def kdev(pos):
        return (sp + (pos - kpos) * kstride, tp)

    def qdev(pos):
        return (sp + (pos - qpos) * qstride, tp)

    def remote(src, dst, ssem, rsem, dev):
        return pltpu.make_async_remote_copy(
            src_ref=src, dst_ref=dst, send_sem=ssem, recv_sem=rsem, device_id=dev, device_id_type=MESH
        )

    prev_sp = (sp + 63) % 64
    next_sp = (sp + 1) % 64

    cp_tok = pltpu.make_async_copy(tok_h, tok.at[tp], lsem.at[0])
    cp_tok.start()
    loads = []
    for i, w in enumerate((wq1_h, wq2_h, wk1_h, wk2_h)):
        loads.append(pltpu.make_async_copy(w, wn.at[pl.ds(KD * i, KD), :], lsem.at[1 + i]))
    for i, w in enumerate((wv_h, wg_h, wo_h, wi_h, wx_h)):
        loads.append(pltpu.make_async_copy(w, wall.at[:, pl.ds(128 * i, 128)], lsem.at[5 + i]))
    my_half = pl.ds(pl.multiple_of(c * HALF, HALF), HALF)
    other_half = pl.ds(pl.multiple_of((1 - c) * HALF, HALF), HALF)
    loads.append(pltpu.make_async_copy(aw_h, wa.at[pl.ds(pl.multiple_of(tp * VD, VD), VD), :], lsem.at[10]))
    loads.append(pltpu.make_async_copy(cw_h.at[:, my_half], wout.at[c], lsem.at[11]))
    for cp in loads:
        cp.start()

    barrier = pltpu.get_barrier_semaphore()

    def greet(dev):
        pl.semaphore_signal(barrier, inc=1, device_id=dev, device_id_type=MESH)

    right_chip = (sp, ((x + 1) % 4) * 2 + c)
    left_chip = (sp, ((x + 3) % 4) * 2 + c)
    partner = (sp, other)
    k_right, k_left = kdev((kpos + 1) % 8), kdev((kpos + 7) % 8)
    q_right, q_left = qdev((qpos + 1) % 8), qdev((qpos + 7) % 8)
    k_right2, k_left2 = kdev((kpos + 2) % 8), kdev((kpos + 6) % 8)
    q_right2, q_left2 = qdev((qpos + 2) % 8), qdev((qpos + 6) % 8)
    greeted = (
        right_chip, left_chip, partner, (prev_sp, tp), (next_sp, tp),
        k_right, k_left, q_right, q_left, k_right2, k_left2, q_right2, q_left2,
    )
    for dev in greeted:
        greet(dev)
    pl.semaphore_wait(barrier, len(greeted))

    pending = []

    def send(src, dst, ssem, rsem, dev):
        cp = remote(src, dst, ssem, rsem, dev)
        cp.start()
        pending.append(cp)

    def arrived(ref, rsem):
        remote(ref, ref, rsem, rsem, partner).wait_recv()

    top, bottom = pl.ds(0, T // 2), pl.ds(T // 2, T // 2)
    halves = (top, bottom)

    def tok_send(t, half, slot, dev):
        ref = tok.at[t, halves[half], :]
        send(ref, ref, tok_s.at[slot], tok_r.at[t, half], dev)

    def tok_wait(t, half):
        arrived(tok.at[t, halves[half], :], tok_r.at[t, half])

    cp_tok.wait()
    tok_send(tp, 0, 0, right_chip)
    tok_send(tp, 1, 1, left_chip)
    tok_send(tp, 1, 2, right_chip)
    tok_send(tp, 0, 3, left_chip)
    tok_send(tp, 0, 4, partner)
    tok_send(tp, 1, 5, partner)

    for cp in loads[:9]:
        cp.wait()

    def project(t, first=False):
        block = tok[t].astype(F32)
        sq = block * block
        sq = sq[:, :128] + sq[:, 128:]
        at = pl.ds(pl.multiple_of(t * FB, FB), FB)
        scaled = (block * gain[:, at]).astype(BF)
        narrow = lax.dot_general(scaled, wn[:, at], (((1,), (1,)), ((), ())), preferred_element_type=F32)
        wide = dot(scaled, wall[at, :])
        if first:
            ss[...] = sq
            acc[:, pl.ds(0, 256)] = narrow
            acc[:, pl.ds(256, 640)] = wide
        else:
            ss[...] += sq
            acc[:, pl.ds(0, 256)] += narrow
            acc[:, pl.ds(256, 640)] += wide

    xl, xr, xo = (x + 3) % 4, (x + 1) % 4, (x + 2) % 4
    oc = 1 - c
    project(tp, True)
    tok_wait(other, 0)
    tok_wait(other, 1)
    project(other)
    tok_wait(xl * 2 + c, 0)
    tok_send(xl * 2 + c, 0, 6, right_chip)
    tok_send(xl * 2 + c, 0, 7, partner)
    tok_wait(xr * 2 + c, 1)
    tok_send(xr * 2 + c, 1, 8, left_chip)
    tok_send(xr * 2 + c, 1, 9, partner)
    tok_wait(xl * 2 + c, 1)
    tok_send(xl * 2 + c, 1, 10, partner)
    tok_wait(xr * 2 + c, 0)
    tok_send(xr * 2 + c, 0, 11, partner)
    project(xl * 2 + c)
    project(xr * 2 + c)
    tok_wait(xl * 2 + oc, 0)
    tok_wait(xl * 2 + oc, 1)
    project(xl * 2 + oc)
    tok_wait(xr * 2 + oc, 0)
    tok_wait(xr * 2 + oc, 1)
    project(xr * 2 + oc)
    tok_wait(xo * 2 + c, 0)
    tok_send(xo * 2 + c, 0, 12, partner)
    tok_wait(xo * 2 + c, 1)
    tok_send(xo * 2 + c, 1, 13, partner)
    project(xo * 2 + c)
    tok_wait(xo * 2 + oc, 0)
    tok_wait(xo * 2 + oc, 1)
    project(xo * 2 + oc)

    quarter = VD // 2

    def wa_part(t, half):
        return wa.at[pl.ds(pl.multiple_of(t * VD + half * quarter, quarter), quarter), :]

    def wa_copy(t, half, slot, dev):
        return remote(wa_part(t, half), wa_part(t, half), wa_s.at[slot], wa_r.at[t, half], dev)

    def wa_send(t, half, slot, dev):
        send(wa_part(t, half), wa_part(t, half), wa_s.at[slot], wa_r.at[t, half], dev)

    def wa_wait(t, half):
        arrived(wa_part(t, half), wa_r.at[t, half])

    for cp in loads[9:]:
        cp.wait()
    wa_send(tp, 0, 0, right_chip)
    wa_send(tp, 1, 1, left_chip)
    wa_send(tp, 1, 2, right_chip)
    wa_send(tp, 0, 3, left_chip)
    wa_send(tp, 0, 4, partner)
    wa_send(tp, 1, 5, partner)

    inv = lax.rsqrt(jnp.sum(ss[...], axis=1, keepdims=True) / D + EPS)

    def k_send(pos, slot, dev):
        send(kb.at[pos], kb.at[pos], k_s.at[slot], k_r.at[pos], dev)

    def v_send(pos, slot, dev):
        send(vb.at[pos], vb.at[pos], v_s.at[slot], v_r.at[pos], dev)

    def q_send(pos, slot, dev):
        send(qb.at[pos], qb.at[pos], q_s.at[slot], q_r.at[pos], dev)

    def q_part(pos, part, slot, dev):
        ref = qb.at[pos, pl.ds(KD * part, KD), :]
        send(ref, ref, q_s.at[slot], q_r.at[pos if part == 0 else 8], dev)

    kb[kpos] = (acc[:, 128:256] * inv).astype(BF)
    for slot, dev in enumerate((k_right2, k_left2, k_right, k_left)):
        k_send(kpos, slot, dev)
    vb[kpos] = (acc[:, 256:384] * inv).T.astype(BF)
    for slot, dev in enumerate((k_left2, k_right2, k_left, k_right)):
        v_send(kpos, slot, dev)
    qb[qpos] = (acc[:, 0:128] * (inv * QSCALE)).T.astype(BF)
    for slot, dev in enumerate((q_right2, q_left2, q_right, q_left)):
        q_send(qpos, slot, dev)

    gate[...] = (acc[:, 384:512] * inv).astype(BF)
    outer[...] = (acc[:, 512:640] * inv).astype(BF)
    pr = ((acc[:, 640:768] * inv).astype(BF).astype(F32) * (acc[:, 768:896] * inv).astype(BF).astype(F32)).astype(BF)
    pr = pr.astype(F32)
    prod[...] = pr
    edge[0] = pr[0:8]
    edge[1] = pr[T - 8 : T]
    to_prev = remote(edge.at[0], halo.at[1], h_s.at[0], h_r.at[1], (prev_sp, tp))
    to_next = remote(edge.at[1], halo.at[0], h_s.at[1], h_r.at[0], (next_sp, tp))
    to_prev.start()
    to_next.start()

    def at(pos, d):
        return (pos + d) % 8

    arrived(kb.at[at(kpos, 6)], k_r.at[at(kpos, 6)])
    k_send(at(kpos, 6), 4, k_right2)
    k_send(at(kpos, 6), 5, k_right)
    arrived(kb.at[at(kpos, 2)], k_r.at[at(kpos, 2)])
    k_send(at(kpos, 2), 6, k_left)
    arrived(vb.at[at(kpos, 2)], v_r.at[at(kpos, 2)])
    v_send(at(kpos, 2), 4, k_left2)
    v_send(at(kpos, 2), 5, k_left)
    arrived(vb.at[at(kpos, 6)], v_r.at[at(kpos, 6)])
    v_send(at(kpos, 6), 6, k_right)
    arrived(qb.at[at(qpos, 6)], q_r.at[at(qpos, 6)])
    q_part(at(qpos, 6), 0, 4, q_right2)
    q_send(at(qpos, 6), 5, q_right)
    arrived(qb.at[at(qpos, 2)], q_r.at[at(qpos, 2)])
    q_part(at(qpos, 2), 1, 6, q_left2)
    q_send(at(qpos, 2), 7, q_left)
    to_prev.wait_recv()
    to_next.wait_recv()
    before = jnp.where(sp == 0, 0.0, halo[0][7:8, :])
    after = jnp.where(sp == 63, 0.0, halo[1][0:1, :])
    cur = prod[...]
    rows = lax.broadcasted_iota(jnp.int32, (T, VD), 0)
    up = jnp.where(rows == 0, before, pltpu.roll(cur, 1, 0))
    down = jnp.where(rows == T - 1, after, pltpu.roll(cur, T - 1, 0))
    tp32 = taps[...].astype(F32)
    conv = tp32[0:1] * up + tp32[1:2] * cur + tp32[2:3] * down
    mix[c] = (outer[...].astype(F32) * conv).astype(BF)

    send(mix.at[c], mix.at[c], m_s, m_r, partner)
    send(cw_h.at[:, other_half], wout.at[c], w_s, w_r, partner)
    arrived(mix.at[1 - c], m_r)
    arrived(wout.at[1 - c], w_r)

    def p_copy(chip, core):
        return remote(
            psend.at[chip, pl.ds(pl.multiple_of(core * ROWS, ROWS), ROWS), :],
            precv.at[tp],
            p_s.at[chip * 2 + core],
            p_r.at[tp],
            (sp, chip * 2 + core),
        )

    def to_chip(i, carry):
        chip = (x + jnp.where(i == 0, 2, jnp.where(i == 1, 1, jnp.where(i == 2, 3, 0)))) % 4
        rows = pl.ds(pl.multiple_of(chip * 2 * ROWS, 2 * ROWS), 2 * ROWS)
        psend[chip] = (dot(mix[0, rows, :], wout[0]) + dot(mix[1, rows, :], wout[1])).astype(BF)

        @pl.when(i < 3)
        def _():
            p_copy(chip, c).start()

        p_copy(chip, 1 - c).start()
        return carry

    lax.fori_loop(0, 4, to_chip, 0)
    precv[tp] = psend[x, pl.ds(pl.multiple_of(c * ROWS, ROWS), ROWS), :]

    for d in (1, 7, 3, 5, 4):
        arrived(kb.at[at(kpos, d)], k_r.at[at(kpos, d)])
        arrived(vb.at[at(kpos, d)], v_r.at[at(kpos, d)])
    for d in (1, 7, 3, 5):
        arrived(qb.at[at(qpos, d)], q_r.at[at(qpos, d)])
    arrived(qb.at[at(qpos, 4), pl.ds(0, KD), :], q_r.at[at(qpos, 4)])
    arrived(qb.at[at(qpos, 4), pl.ds(KD, KD), :], q_r.at[8])

    def wa_forward():
        for slot, (t, half, dev) in enumerate((
            (xl * 2 + c, 0, right_chip), (xr * 2 + c, 1, left_chip), (xl * 2 + c, 1, None), (xr * 2 + c, 0, None)
        )):
            wa_wait(t, half)
            if dev is not None:
                wa_copy(t, half, 6 + slot, dev).start()
            wa_copy(t, half, 8 + slot, partner).start()

    zero = jnp.zeros((KD, T), BF)

    def scores(qm, n, s_ref, peak):
        s = dot(kb[n], qm)
        s_ref[pl.ds(n * T, T), :] = s
        top = jnp.max(s.reshape(T // 8, 8, T), axis=0)
        return top if peak is None else jnp.maximum(peak, top)

    def apply(n, s_ref, peak, state):
        p = jnp.exp2(s_ref[pl.ds(n * T, T), :] - peak)
        part = jnp.sum(p.reshape(T // 8, 8, T), axis=0)
        o = dot(vb[n], p.astype(BF))
        return (part, o) if state is None else (state[0] + part, state[1] + o)

    def one_block(i, carry):
        odd = i % 2
        mag = 4 - (i + 1) // 2
        off = odd * mag + (1 - odd) * ((8 - mag) % 8)
        pos = (qpos + off) % 8

        pl.when(i == 2)(wa_forward)

        q = qb[pos]
        q1 = jnp.concatenate([q[:KD], zero], axis=0)
        q2 = jnp.concatenate([zero, q[KD:]], axis=0)
        peak = None
        for n in range(R):
            peak = scores(q1, n, s1, peak)
        peak1 = jnp.max(peak, axis=0, keepdims=True)
        peak = None
        state = None
        for n in range(R):
            peak = scores(q2, n, s2, peak)
            state = apply(n, s1, peak1, state)
        peak2 = jnp.max(peak, axis=0, keepdims=True)
        sum1 = jnp.sum(state[0], axis=0, keepdims=True)
        osend[pos, pl.ds(0, VD), :] = state[1].astype(BF)
        state = None
        for n in range(R):
            state = apply(n, s2, peak2, state)
        sum2 = jnp.sum(state[0], axis=0, keepdims=True)
        osend[pos, pl.ds(VD, VD), :] = state[1].astype(BF)
        tsend[pos] = jnp.concatenate([peak1, sum1, peak2, sum2, peak1, sum1, peak2, sum2], axis=0)

        @pl.when(i < 7)
        def _():
            remote(osend.at[pos], orecv.at[qpos], o_s.at[pos], o_r.at[qpos], qdev(pos)).start()
            remote(tsend.at[pos], trecv.at[qpos], st_s.at[pos], st_r.at[qpos], qdev(pos)).start()

        return carry

    lax.fori_loop(0, 8, one_block, 0)

    orecv[qpos] = osend[qpos]
    trecv[qpos] = tsend[qpos]

    wa_wait(xo * 2 + c, 0)
    wa_send(xo * 2 + c, 0, 12, partner)
    wa_wait(xo * 2 + c, 1)
    wa_send(xo * 2 + c, 1, 13, partner)

    def p_wait(d, carry):
        src = (tp + d) % 8
        arrived(precv.at[src], p_r.at[src])
        return carry

    lax.fori_loop(1, 8, p_wait, 0)
    for half in range(2):
        total = precv[half].astype(F32)
        for n in range(1, 4):
            total += precv[2 * n + half].astype(F32)
        csum[:, pl.ds(half * HALF, HALF)] = total
    for t in (other, xl * 2 + oc, xr * 2 + oc, xo * 2 + oc):
        wa_wait(t, 0)
        wa_wait(t, 1)

    def o_wait(d, carry):
        pos = (qpos + d) % 8
        remote(osend.at[pos], orecv.at[pos], o_s.at[pos], o_r.at[pos], qdev(pos)).wait_recv()
        remote(tsend.at[pos], trecv.at[pos], st_s.at[pos], st_r.at[pos], qdev(pos)).wait_recv()
        return carry

    lax.fori_loop(1, 8, o_wait, 0)

    def merged(row, at):
        peak = trecv[0, pl.ds(row, 1), :]
        for n in range(1, R):
            peak = jnp.maximum(peak, trecv[n, pl.ds(row, 1), :])
        total = None
        for n in range(R):
            w = jnp.exp2(trecv[n, pl.ds(row, 1), :] - peak)
            part = w * trecv[n, pl.ds(row + 1, 1), :]
            o = w * orecv[n, pl.ds(at, VD), :].astype(F32)
            total = (part, o) if total is None else (total[0] + part, total[1] + o)
        return total[1] / total[0]

    diff = merged(0, 0) - lam[0] * merged(2, VD)
    diff = (diff * lax.rsqrt(jnp.mean(diff * diff, axis=0, keepdims=True) + EPS)).T
    g32 = gate[...].astype(F32)
    amix[...] = (diff * hgain[...] * (g32 / (1.0 + jnp.exp(-g32)))).astype(BF)

    mine = pl.ds(pl.multiple_of(tp * VD, VD), VD)

    def a_copy(t):
        rows = pl.ds(pl.multiple_of(t * ROWS, ROWS), ROWS)
        return remote(amix.at[rows, :], arecv.at[:, mine], a_s.at[t], a_r.at[tp], (sp, t))

    for e in (4, 5, 3, 2, 6, 1, 7):
        a_copy((tp + e) % 8).start()
    arecv[:, mine] = amix[pl.ds(pl.multiple_of(tp * ROWS, ROWS), ROWS), :]
    for e in (1, 7, 2, 6, 3, 5, 4):
        src = (tp + e) % 8
        arrived(arecv.at[:, pl.ds(pl.multiple_of(src * VD, VD), VD)], a_r.at[src])
    for n in range(4):
        cols = pl.ds(n * 512, 512)
        out[:, cols] = (dot(arecv[...], wa[:, cols]) + csum[:, cols]).astype(BF)

    for cp in pending:
        cp.wait_send()
    for slot in range(6, 12):
        wa_copy(tp, 0, slot, partner).wait_send()
    for d in range(1, 8):
        pos = (qpos + d) % 8
        remote(osend.at[pos], orecv.at[qpos], o_s.at[pos], o_r.at[qpos], qdev(pos)).wait_send()
        remote(tsend.at[pos], trecv.at[qpos], st_s.at[pos], st_r.at[qpos], qdev(pos)).wait_send()
        dst = (tp + d) % 8
        p_copy(dst // 2, dst % 2).wait_send()
        a_copy(dst).wait_send()
    to_prev.wait_send()
    to_next.wait_send()


def local(tokens, norm_gain, q1, k1, q2, k2, wv, wg, wo, wi, wx, taps, lam, hgain, aw, cw):
    hbm = pl.BlockSpec(memory_space=pltpu.HBM)
    vm = pl.BlockSpec(memory_space=pltpu.VMEM)
    sm = pl.BlockSpec(memory_space=pltpu.SMEM)
    dma = pltpu.SemaphoreType.DMA
    v = pltpu.VMEM
    return pl.pallas_call(
        kernel,
        out_shape=jax.ShapeDtypeStruct((ROWS, D), BF),
        in_specs=[hbm, vm] + [hbm] * 9 + [vm, sm, vm, hbm, hbm],
        out_specs=vm,
        scratch_shapes=[
            v((8, T, FB), BF), v((4 * KD, D), BF), v((D, 640), BF), v((T, 896), F32), v((T, 128), F32),
            v((R, T, 128), BF), v((R, VD, T), BF), v((R, 128, T), BF),
            v((T, VD), BF), v((T, VD), BF), v((T, VD), F32), v((2, 8, VD), F32), v((2, 8, VD), F32),
            v((KEYS, T), F32), v((KEYS, T), F32),
            v((R, 2 * VD, T), BF), v((R, 2 * VD, T), BF), v((R, 8, T), F32), v((R, 8, T), F32),
            v((2, T, VD), BF), v((2, VD, HALF), BF), v((4, 2 * ROWS, HALF), BF), v((8, ROWS, HALF), BF),
            v((8 * VD, D), BF), v((ROWS, D), F32), v((T, VD), BF), v((ROWS, 8 * VD), BF),
            dma((12,)), dma((14,)), dma((8, 2)), dma((8,)), dma((8,)), dma((8,)), dma((8,)), dma((8,)), dma((9,)),
            dma((8,)), dma((8,)), dma((8,)), dma((8,)), dma((2,)), dma((2,)), dma, dma, dma, dma,
            dma((8,)), dma((8,)), dma((14,)), dma((8, 2)), dma((8,)), dma((8,)),
        ],
        compiler_params=pltpu.CompilerParams(
            collective_id=0, has_side_effects=True, vmem_limit_bytes=67043328
        ),
        name="layer",
    )(tokens, norm_gain.reshape(1, D), q1.T, k1.T, q2.T, k2.T, wv, wg, wo, wi, wx, taps, lam, hgain.reshape(1, VD), aw, cw)


def solution(mesh):
    col = P(None, "tp")
    return jax.shard_map(
        local,
        mesh=mesh,
        in_specs=(P("sp", "tp"), P()) + (col,) * 10 + (P("tp"), P(), P("tp", None), P("tp", None)),
        out_specs=P(("sp", "tp"), None),
        check_vma=False,
    )
```

```python
import math

import jax
import jax.numpy as jnp
from jax import lax
from jax.experimental import pallas as pl
from jax.experimental.pallas import tpu as pltpu
from jax.sharding import PartitionSpec as P

MESH = pl.DeviceIdType.MESH
EPS = 1e-06
BF = jnp.bfloat16
F32 = jnp.float32
T, FB, D, R, KD, VD = 256, 256, 2048, 8, 64, 128
NTP = 8
KEYS = R * T
HALF = D // 2
ROWS = T // NTP
QSCALE = math.log2(math.e) / math.sqrt(KD)


def dot(a, b):
    return jnp.dot(a, b, preferred_element_type=F32)


def kernel(
    tok_h, gain, wq1_h, wk1_h, wq2_h, wk2_h, wv_h, wg_h, wo_h, wi_h, wx_h, taps, lam, hgain, aw_h, cw_h,
    out,
    tok, wn, wall, acc, ss, kb, vb, qb, gate, outer, prod, edge, halo, s1, s2, osend, orecv, tsend, trecv,
    mix, wout, psend, precv, wa, csum, amix, arecv, ms, mo,
    lsem, tok_s, tok_r, k_s, k_r, v_s, v_r, q_s, q_r, o_s, o_r, st_s, st_r, h_s, h_r, m_s, m_r, w_s, w_r, p_s, p_r, wa_s, wa_r, a_s, a_r,
):
    sp = lax.axis_index("sp")
    tp = lax.axis_index("tp")
    c = tp % 2
    x = tp // 2
    z = sp // 8
    y = sp % 8
    kpos = (1 - c) * z + c * y
    qpos = (1 - c) * y + c * z
    kstride = 8 - 7 * c
    qstride = 1 + 7 * c
    other = x * 2 + 1 - c

    def kdev(pos):
        return (sp + (pos - kpos) * kstride, tp)

    def qdev(pos):
        return (sp + (pos - qpos) * qstride, tp)

    def remote(src, dst, ssem, rsem, dev):
        return pltpu.make_async_remote_copy(
            src_ref=src, dst_ref=dst, send_sem=ssem, recv_sem=rsem, device_id=dev, device_id_type=MESH
        )

    prev_sp = (sp + 63) % 64
    next_sp = (sp + 1) % 64

    cp_tok = pltpu.make_async_copy(tok_h, tok.at[tp], lsem.at[0])
    cp_tok.start()
    loads = []
    for i, w in enumerate((wq1_h, wq2_h, wk1_h, wk2_h)):
        loads.append(pltpu.make_async_copy(w, wn.at[pl.ds(KD * i, KD), :], lsem.at[1 + i]))
    for i, w in enumerate((wv_h, wg_h, wo_h, wi_h, wx_h)):
        loads.append(pltpu.make_async_copy(w, wall.at[:, pl.ds(128 * i, 128)], lsem.at[5 + i]))
    my_half = pl.ds(pl.multiple_of(c * HALF, HALF), HALF)
    other_half = pl.ds(pl.multiple_of((1 - c) * HALF, HALF), HALF)
    loads.append(pltpu.make_async_copy(aw_h, wa.at[pl.ds(pl.multiple_of(tp * VD, VD), VD), :], lsem.at[10]))
    loads.append(pltpu.make_async_copy(cw_h.at[:, my_half], wout.at[c], lsem.at[11]))
    for cp in loads:
        cp.start()

    barrier = pltpu.get_barrier_semaphore()

    def greet(dev):
        pl.semaphore_signal(barrier, inc=1, device_id=dev, device_id_type=MESH)

    right_chip = (sp, ((x + 1) % 4) * 2 + c)
    left_chip = (sp, ((x + 3) % 4) * 2 + c)
    partner = (sp, other)
    k_right, k_left = kdev((kpos + 1) % 8), kdev((kpos + 7) % 8)
    q_right, q_left = qdev((qpos + 1) % 8), qdev((qpos + 7) % 8)
    k_right2, k_left2 = kdev((kpos + 2) % 8), kdev((kpos + 6) % 8)
    q_right2, q_left2 = qdev((qpos + 2) % 8), qdev((qpos + 6) % 8)
    greeted = (
        right_chip, left_chip, partner, (prev_sp, tp), (next_sp, tp),
        k_right, k_left, q_right, q_left, k_right2, k_left2, q_right2, q_left2,
    )
    for dev in greeted:
        greet(dev)
    pl.semaphore_wait(barrier, len(greeted))

    pending = []

    def send(src, dst, ssem, rsem, dev):
        cp = remote(src, dst, ssem, rsem, dev)
        cp.start()
        pending.append(cp)

    def arrived(ref, rsem):
        remote(ref, ref, rsem, rsem, partner).wait_recv()

    top, bottom = pl.ds(0, T // 2), pl.ds(T // 2, T // 2)
    halves = (top, bottom)

    def tok_send(t, half, slot, dev):
        ref = tok.at[t, halves[half], :]
        send(ref, ref, tok_s.at[slot], tok_r.at[t, half], dev)

    def tok_wait(t, half):
        arrived(tok.at[t, halves[half], :], tok_r.at[t, half])

    cp_tok.wait()
    tok_send(tp, 0, 0, right_chip)
    tok_send(tp, 1, 1, left_chip)
    tok_send(tp, 1, 2, right_chip)
    tok_send(tp, 0, 3, left_chip)
    tok_send(tp, 0, 4, partner)
    tok_send(tp, 1, 5, partner)

    for cp in loads[:9]:
        cp.wait()

    def project(t, first=False):
        block = tok[t].astype(F32)
        sq = block * block
        sq = sq[:, :128] + sq[:, 128:]
        at = pl.ds(pl.multiple_of(t * FB, FB), FB)
        scaled = (block * gain[:, at]).astype(BF)
        narrow = lax.dot_general(scaled, wn[:, at], (((1,), (1,)), ((), ())), preferred_element_type=F32)
        wide = dot(scaled, wall[at, :])
        if first:
            ss[...] = sq
            acc[:, pl.ds(0, 256)] = narrow
            acc[:, pl.ds(256, 640)] = wide
        else:
            ss[...] += sq
            acc[:, pl.ds(0, 256)] += narrow
            acc[:, pl.ds(256, 640)] += wide

    xl, xr, xo = (x + 3) % 4, (x + 1) % 4, (x + 2) % 4
    oc = 1 - c
    project(tp, True)
    tok_wait(other, 0)
    tok_wait(other, 1)
    project(other)
    tok_wait(xl * 2 + c, 0)
    tok_send(xl * 2 + c, 0, 6, right_chip)
    tok_send(xl * 2 + c, 0, 7, partner)
    tok_wait(xr * 2 + c, 1)
    tok_send(xr * 2 + c, 1, 8, left_chip)
    tok_send(xr * 2 + c, 1, 9, partner)
    tok_wait(xl * 2 + c, 1)
    tok_send(xl * 2 + c, 1, 10, partner)
    tok_wait(xr * 2 + c, 0)
    tok_send(xr * 2 + c, 0, 11, partner)
    project(xl * 2 + c)
    project(xr * 2 + c)
    tok_wait(xl * 2 + oc, 0)
    tok_wait(xl * 2 + oc, 1)
    project(xl * 2 + oc)
    tok_wait(xr * 2 + oc, 0)
    tok_wait(xr * 2 + oc, 1)
    project(xr * 2 + oc)
    tok_wait(xo * 2 + c, 0)
    tok_send(xo * 2 + c, 0, 12, partner)
    tok_wait(xo * 2 + c, 1)
    tok_send(xo * 2 + c, 1, 13, partner)
    project(xo * 2 + c)
    tok_wait(xo * 2 + oc, 0)
    tok_wait(xo * 2 + oc, 1)
    project(xo * 2 + oc)

    quarter = VD // 2

    def wa_part(t, half):
        return wa.at[pl.ds(pl.multiple_of(t * VD + half * quarter, quarter), quarter), :]

    def wa_copy(t, half, slot, dev):
        return remote(wa_part(t, half), wa_part(t, half), wa_s.at[slot], wa_r.at[t, half], dev)

    def wa_send(t, half, slot, dev):
        send(wa_part(t, half), wa_part(t, half), wa_s.at[slot], wa_r.at[t, half], dev)

    def wa_wait(t, half):
        arrived(wa_part(t, half), wa_r.at[t, half])

    for cp in loads[9:]:
        cp.wait()
    wa_send(tp, 0, 0, right_chip)
    wa_send(tp, 1, 1, left_chip)
    wa_send(tp, 1, 2, right_chip)
    wa_send(tp, 0, 3, left_chip)
    wa_send(tp, 0, 4, partner)
    wa_send(tp, 1, 5, partner)

    inv = lax.rsqrt(jnp.sum(ss[...], axis=1, keepdims=True) / D + EPS)

    def k_send(pos, slot, dev):
        send(kb.at[pos], kb.at[pos], k_s.at[slot], k_r.at[pos], dev)

    def v_send(pos, slot, dev):
        send(vb.at[pos], vb.at[pos], v_s.at[slot], v_r.at[pos], dev)

    def q_send(pos, slot, dev):
        send(qb.at[pos], qb.at[pos], q_s.at[slot], q_r.at[pos], dev)

    def q_part(pos, part, slot, dev):
        ref = qb.at[pos, pl.ds(KD * part, KD), :]
        send(ref, ref, q_s.at[slot], q_r.at[pos if part == 0 else 8], dev)

    kb[kpos] = (acc[:, 128:256] * inv).astype(BF)
    for slot, dev in enumerate((k_right2, k_left2, k_right, k_left)):
        k_send(kpos, slot, dev)
    vb[kpos] = (acc[:, 256:384] * inv).T.astype(BF)
    for slot, dev in enumerate((k_left2, k_right2, k_left, k_right)):
        v_send(kpos, slot, dev)
    qb[qpos] = (acc[:, 0:128] * (inv * QSCALE)).T.astype(BF)
    for slot, dev in enumerate((q_right2, q_left2, q_right, q_left)):
        q_send(qpos, slot, dev)

    gate[...] = (acc[:, 384:512] * inv).astype(BF)
    outer[...] = (acc[:, 512:640] * inv).astype(BF)
    pr = ((acc[:, 640:768] * inv).astype(BF).astype(F32) * (acc[:, 768:896] * inv).astype(BF).astype(F32)).astype(BF)
    pr = pr.astype(F32)
    prod[...] = pr
    edge[0] = pr[0:8]
    edge[1] = pr[T - 8 : T]
    to_prev = remote(edge.at[0], halo.at[1], h_s.at[0], h_r.at[1], (prev_sp, tp))
    to_next = remote(edge.at[1], halo.at[0], h_s.at[1], h_r.at[0], (next_sp, tp))
    to_prev.start()
    to_next.start()

    def at(pos, d):
        return (pos + d) % 8

    arrived(kb.at[at(kpos, 6)], k_r.at[at(kpos, 6)])
    k_send(at(kpos, 6), 4, k_right2)
    k_send(at(kpos, 6), 5, k_right)
    arrived(kb.at[at(kpos, 2)], k_r.at[at(kpos, 2)])
    k_send(at(kpos, 2), 6, k_left)
    arrived(vb.at[at(kpos, 2)], v_r.at[at(kpos, 2)])
    v_send(at(kpos, 2), 4, k_left2)
    v_send(at(kpos, 2), 5, k_left)
    arrived(vb.at[at(kpos, 6)], v_r.at[at(kpos, 6)])
    v_send(at(kpos, 6), 6, k_right)
    arrived(qb.at[at(qpos, 6)], q_r.at[at(qpos, 6)])
    q_part(at(qpos, 6), 0, 4, q_right2)
    q_send(at(qpos, 6), 5, q_right)
    arrived(qb.at[at(qpos, 2)], q_r.at[at(qpos, 2)])
    q_part(at(qpos, 2), 1, 6, q_left2)
    q_send(at(qpos, 2), 7, q_left)
    to_prev.wait_recv()
    to_next.wait_recv()
    before = jnp.where(sp == 0, 0.0, halo[0][7:8, :])
    after = jnp.where(sp == 63, 0.0, halo[1][0:1, :])
    cur = prod[...]
    rows = lax.broadcasted_iota(jnp.int32, (T, VD), 0)
    up = jnp.where(rows == 0, before, pltpu.roll(cur, 1, 0))
    down = jnp.where(rows == T - 1, after, pltpu.roll(cur, T - 1, 0))
    tp32 = taps[...].astype(F32)
    conv = tp32[0:1] * up + tp32[1:2] * cur + tp32[2:3] * down
    mix[c] = (outer[...].astype(F32) * conv).astype(BF)

    send(mix.at[c], mix.at[c], m_s, m_r, partner)
    send(cw_h.at[:, other_half], wout.at[c], w_s, w_r, partner)
    arrived(mix.at[1 - c], m_r)
    arrived(wout.at[1 - c], w_r)

    def p_copy(chip, core):
        return remote(
            psend.at[chip, pl.ds(pl.multiple_of(core * ROWS, ROWS), ROWS), :],
            precv.at[tp],
            p_s.at[chip * 2 + core],
            p_r.at[tp],
            (sp, chip * 2 + core),
        )

    def to_chip(i, carry):
        chip = (x + jnp.where(i == 0, 2, jnp.where(i == 1, 1, jnp.where(i == 2, 3, 0)))) % 4
        rows = pl.ds(pl.multiple_of(chip * 2 * ROWS, 2 * ROWS), 2 * ROWS)
        psend[chip] = (dot(mix[0, rows, :], wout[0]) + dot(mix[1, rows, :], wout[1])).astype(BF)

        @pl.when(i < 3)
        def _():
            p_copy(chip, c).start()

        p_copy(chip, 1 - c).start()
        return carry

    lax.fori_loop(0, 4, to_chip, 0)
    precv[tp] = psend[x, pl.ds(pl.multiple_of(c * ROWS, ROWS), ROWS), :]

    wa_wait(xl * 2 + c, 0)
    wa_send(xl * 2 + c, 0, 6, right_chip)
    wa_send(xl * 2 + c, 0, 8, partner)
    wa_wait(xr * 2 + c, 1)
    wa_send(xr * 2 + c, 1, 7, left_chip)
    wa_send(xr * 2 + c, 1, 9, partner)

    for d in (1, 7, 3, 5, 4):
        arrived(kb.at[at(kpos, d)], k_r.at[at(kpos, d)])
        arrived(vb.at[at(kpos, d)], v_r.at[at(kpos, d)])
    for d in (1, 7, 3, 5):
        arrived(qb.at[at(qpos, d)], q_r.at[at(qpos, d)])
    arrived(qb.at[at(qpos, 4), pl.ds(0, KD), :], q_r.at[at(qpos, 4)])
    arrived(qb.at[at(qpos, 4), pl.ds(KD, KD), :], q_r.at[8])

    def wa_forward():
        for slot, (t, half) in enumerate(((xl * 2 + c, 1), (xr * 2 + c, 0))):
            wa_wait(t, half)
            wa_copy(t, half, 10 + slot, partner).start()

    zero = jnp.zeros((KD, T), BF)

    def scores(qm, n, s_ref, peak):
        s = dot(kb[n], qm)
        s_ref[pl.ds(n * T, T), :] = s
        top = jnp.max(s.reshape(T // 8, 8, T), axis=0)
        return top if peak is None else jnp.maximum(peak, top)

    def apply(n, s_ref, peak, state):
        p = jnp.exp2(s_ref[pl.ds(n * T, T), :] - peak)
        part = jnp.sum(p.reshape(T // 8, 8, T), axis=0)
        o = dot(vb[n], p.astype(BF))
        return (part, o) if state is None else (state[0] + part, state[1] + o)

    def ring_place(i):
        odd = i % 2
        mag = 4 - (i + 1) // 2
        return (qpos + odd * mag + (1 - odd) * ((8 - mag) % 8)) % 8

    def first_map(pos):
        return jnp.concatenate([qb[pos, pl.ds(0, KD), :], zero], axis=0)

    def second_map(pos):
        return jnp.concatenate([zero, qb[pos, pl.ds(KD, KD), :]], axis=0)

    def one_block(i, peak1):
        pos = ring_place(i)
        pl.when(i == 2)(wa_forward)
        q2 = second_map(pos)
        peak = None
        state = None
        for n in range(R):
            peak = scores(q2, n, s2, peak)
            state = apply(n, s1, peak1, state)
        peak2 = jnp.max(peak, axis=0, keepdims=True)
        sum1 = jnp.sum(state[0], axis=0, keepdims=True)
        osend[pos, pl.ds(0, VD), :] = state[1].astype(BF)
        q1 = first_map(ring_place((i + 1) % 8))
        peak = None
        state = None
        for n in range(R):
            peak = scores(q1, n, s1, peak)
            state = apply(n, s2, peak2, state)
        next1 = jnp.max(peak, axis=0, keepdims=True)
        sum2 = jnp.sum(state[0], axis=0, keepdims=True)
        osend[pos, pl.ds(VD, VD), :] = state[1].astype(BF)
        tsend[pos] = jnp.concatenate([peak1, sum1, peak2, sum2, peak1, sum1, peak2, sum2], axis=0)

        @pl.when(i < 7)
        def _():
            remote(osend.at[pos], orecv.at[qpos], o_s.at[pos], o_r.at[qpos], qdev(pos)).start()
            remote(tsend.at[pos], trecv.at[qpos], st_s.at[pos], st_r.at[qpos], qdev(pos)).start()

        return next1

    q1 = first_map(ring_place(0))
    peak = None
    for n in range(R):
        peak = scores(q1, n, s1, peak)
    lax.fori_loop(0, 8, one_block, jnp.max(peak, axis=0, keepdims=True))

    orecv[qpos] = osend[qpos]
    trecv[qpos] = tsend[qpos]

    wa_wait(xo * 2 + c, 0)
    wa_send(xo * 2 + c, 0, 12, partner)
    wa_wait(xo * 2 + c, 1)
    wa_send(xo * 2 + c, 1, 13, partner)

    def p_wait(d, carry):
        src = (tp + d) % 8
        arrived(precv.at[src], p_r.at[src])
        return carry

    lax.fori_loop(1, 8, p_wait, 0)
    for half in range(2):
        total = precv[half].astype(F32)
        for n in range(1, 4):
            total += precv[2 * n + half].astype(F32)
        csum[:, pl.ds(half * HALF, HALF)] = total
    for t in (other, xl * 2 + oc, xr * 2 + oc, xo * 2 + oc):
        wa_wait(t, 0)
        wa_wait(t, 1)

    def part(n):
        t = trecv[n]
        return [
            (t[2 * m : 2 * m + 1], t[2 * m + 1 : 2 * m + 2], orecv[n, pl.ds(m * VD, VD), :].astype(F32))
            for m in range(2)
        ]

    def merge(a, b):
        peak = jnp.maximum(a[0], b[0])
        wa_, wb_ = jnp.exp2(a[0] - peak), jnp.exp2(b[0] - peak)
        return peak, wa_ * a[1] + wb_ * b[1], wa_ * a[2] + wb_ * b[2]

    def take(d, state):
        pos = (qpos + d) % 8
        arrived(orecv.at[pos], o_r.at[pos])
        arrived(trecv.at[pos], st_r.at[pos])
        return [merge(a, b) for a, b in zip(state, part(pos))]

    def take_loop(d, carry):
        for m, (peak, total, o) in enumerate(take(d, [(ms[2 * m], ms[2 * m + 1], mo[m]) for m in range(2)])):
            ms[2 * m] = peak
            ms[2 * m + 1] = total
            mo[m] = o
        return carry

    for m, (peak, total, o) in enumerate(part(qpos)):
        ms[2 * m] = peak
        ms[2 * m + 1] = total
        mo[m] = o
    lax.fori_loop(0, 7, lambda i, carry: take_loop((4 + i + i // 4) % 8, carry), 0)
    diff = mo[0] / ms[1] - lam[0] * (mo[1] / ms[3])
    diff = (diff * lax.rsqrt(jnp.mean(diff * diff, axis=0, keepdims=True) + EPS)).T
    g32 = gate[...].astype(F32)
    amix[...] = (diff * hgain[...] * (g32 / (1.0 + jnp.exp(-g32)))).astype(BF)

    mine = pl.ds(pl.multiple_of(tp * VD, VD), VD)

    def a_copy(t):
        rows = pl.ds(pl.multiple_of(t * ROWS, ROWS), ROWS)
        return remote(amix.at[rows, :], arecv.at[:, mine], a_s.at[t], a_r.at[tp], (sp, t))

    for e in (4, 5, 3, 2, 6, 1, 7):
        a_copy((tp + e) % 8).start()
    arecv[:, mine] = amix[pl.ds(pl.multiple_of(tp * ROWS, ROWS), ROWS), :]
    def add_head(t):
        cols = pl.ds(pl.multiple_of(t * VD, VD), VD)
        csum[...] += dot(arecv[:, cols], wa[cols, :])

    add_head(tp)
    for t in (other, xl * 2 + c, xl * 2 + oc, xr * 2 + c, xr * 2 + oc, xo * 2 + c, xo * 2 + oc):
        arrived(arecv.at[:, pl.ds(pl.multiple_of(t * VD, VD), VD)], a_r.at[t])
        add_head(t)
    out[...] = csum[...].astype(BF)

    for cp in pending:
        cp.wait_send()
    for slot in (10, 11):
        wa_copy(tp, 0, slot, partner).wait_send()
    for d in range(1, 8):
        pos = (qpos + d) % 8
        remote(osend.at[pos], orecv.at[qpos], o_s.at[pos], o_r.at[qpos], qdev(pos)).wait_send()
        remote(tsend.at[pos], trecv.at[qpos], st_s.at[pos], st_r.at[qpos], qdev(pos)).wait_send()
        dst = (tp + d) % 8
        p_copy(dst // 2, dst % 2).wait_send()
        a_copy(dst).wait_send()
    to_prev.wait_send()
    to_next.wait_send()


def local(tokens, norm_gain, q1, k1, q2, k2, wv, wg, wo, wi, wx, taps, lam, hgain, aw, cw):
    hbm = pl.BlockSpec(memory_space=pltpu.HBM)
    vm = pl.BlockSpec(memory_space=pltpu.VMEM)
    sm = pl.BlockSpec(memory_space=pltpu.SMEM)
    dma = pltpu.SemaphoreType.DMA
    v = pltpu.VMEM
    return pl.pallas_call(
        kernel,
        out_shape=jax.ShapeDtypeStruct((ROWS, D), BF),
        in_specs=[hbm, vm] + [hbm] * 9 + [vm, sm, vm, hbm, hbm],
        out_specs=vm,
        scratch_shapes=[
            v((8, T, FB), BF), v((4 * KD, D), BF), v((D, 640), BF), v((T, 896), F32), v((T, 128), F32),
            v((R, T, 128), BF), v((R, VD, T), BF), v((R, 128, T), BF),
            v((T, VD), BF), v((T, VD), BF), v((T, VD), F32), v((2, 8, VD), F32), v((2, 8, VD), F32),
            v((KEYS, T), F32), v((KEYS, T), F32),
            v((R, 2 * VD, T), BF), v((R, 2 * VD, T), BF), v((R, 8, T), F32), v((R, 8, T), F32),
            v((2, T, VD), BF), v((2, VD, HALF), BF), v((4, 2 * ROWS, HALF), BF), v((8, ROWS, HALF), BF),
            v((8 * VD, D), BF), v((ROWS, D), F32), v((T, VD), BF), v((ROWS, 8 * VD), BF),
            v((4, 1, T), F32), v((2, VD, T), F32),
            dma((12,)), dma((14,)), dma((8, 2)), dma((8,)), dma((8,)), dma((8,)), dma((8,)), dma((8,)), dma((9,)),
            dma((8,)), dma((8,)), dma((8,)), dma((8,)), dma((2,)), dma((2,)), dma, dma, dma, dma,
            dma((8,)), dma((8,)), dma((14,)), dma((8, 2)), dma((8,)), dma((8,)),
        ],
        compiler_params=pltpu.CompilerParams(
            collective_id=0, has_side_effects=True, vmem_limit_bytes=66500000
        ),
        name="layer",
    )(tokens, norm_gain.reshape(1, D), q1.T, k1.T, q2.T, k2.T, wv, wg, wo, wi, wx, taps, lam, hgain.reshape(1, VD), aw, cw)


def solution(mesh):
    col = P(None, "tp")
    return jax.shard_map(
        local,
        mesh=mesh,
        in_specs=(P("sp", "tp"), P()) + (col,) * 10 + (P("tp"), P(), P("tp", None), P("tp", None)),
        out_specs=P(("sp", "tp"), None),
        check_vma=False,
    )
```

```python
import math

import jax
import jax.numpy as jnp
from jax import lax
from jax.experimental import pallas as pl
from jax.experimental.pallas import tpu as pltpu
from jax.sharding import PartitionSpec as P

MESH = pl.DeviceIdType.MESH
EPS = 1e-06
BF = jnp.bfloat16
F32 = jnp.float32
T, FB, D, R, KD, VD = 256, 256, 2048, 8, 64, 128
NTP = 8
KEYS = R * T
HALF = D // 2
ROWS = T // NTP
QSCALE = math.log2(math.e) / math.sqrt(KD)


def dot(a, b):
    return jnp.dot(a, b, preferred_element_type=F32)


def kernel(
    tok_h, gain, wq1_h, wk1_h, wq2_h, wk2_h, wv_h, wg_h, wo_h, wi_h, wx_h, taps, lam, hgain, aw_h, cw_h,
    out,
    tok, wn, wall, acc, ss, kb, vb, qb, gate, outer, prod, edge, halo, s1, s2, osend, orecv, tsend, trecv,
    mix, wout, psend, precv, wa, csum, amix, arecv, ms, mo, rin, rstat,
    lsem, tok_s, tok_r, k_s, k_r, v_s, v_r, q_s, q_r, o_s, o_r, st_s, st_r, h_s, h_r, m_s, m_r, w_s, w_r, p_s, p_r, wa_s, wa_r, a_s, a_r, x_s, x_r,
):
    sp = lax.axis_index("sp")
    tp = lax.axis_index("tp")
    c = tp % 2
    x = tp // 2
    z = sp // 8
    y = sp % 8
    kpos = (1 - c) * z + c * y
    qpos = (1 - c) * y + c * z
    kstride = 8 - 7 * c
    qstride = 1 + 7 * c
    other = x * 2 + 1 - c

    def kdev(pos):
        return (sp + (pos - kpos) * kstride, tp)

    def qdev(pos):
        return (sp + (pos - qpos) * qstride, tp)

    def remote(src, dst, ssem, rsem, dev):
        return pltpu.make_async_remote_copy(
            src_ref=src, dst_ref=dst, send_sem=ssem, recv_sem=rsem, device_id=dev, device_id_type=MESH
        )

    prev_sp = (sp + 63) % 64
    next_sp = (sp + 1) % 64

    cp_tok = pltpu.make_async_copy(tok_h, tok.at[tp], lsem.at[0])
    cp_tok.start()
    loads = []
    for i, w in enumerate((wq1_h, wq2_h, wk1_h, wk2_h)):
        loads.append(pltpu.make_async_copy(w, wn.at[pl.ds(KD * i, KD), :], lsem.at[1 + i]))
    for i, w in enumerate((wv_h, wg_h, wo_h, wi_h, wx_h)):
        loads.append(pltpu.make_async_copy(w, wall.at[:, pl.ds(128 * i, 128)], lsem.at[5 + i]))
    my_half = pl.ds(pl.multiple_of(c * HALF, HALF), HALF)
    other_half = pl.ds(pl.multiple_of((1 - c) * HALF, HALF), HALF)
    loads.append(pltpu.make_async_copy(aw_h, wa.at[pl.ds(pl.multiple_of(tp * VD, VD), VD), :], lsem.at[10]))
    loads.append(pltpu.make_async_copy(cw_h.at[:, my_half], wout.at[c], lsem.at[11]))
    for cp in loads:
        cp.start()

    barrier = pltpu.get_barrier_semaphore()

    def greet(dev):
        pl.semaphore_signal(barrier, inc=1, device_id=dev, device_id_type=MESH)

    right_chip = (sp, ((x + 1) % 4) * 2 + c)
    left_chip = (sp, ((x + 3) % 4) * 2 + c)
    partner = (sp, other)
    k_right, k_left = kdev((kpos + 1) % 8), kdev((kpos + 7) % 8)
    q_right, q_left = qdev((qpos + 1) % 8), qdev((qpos + 7) % 8)
    k_right2, k_left2 = kdev((kpos + 2) % 8), kdev((kpos + 6) % 8)
    q_right2, q_left2 = qdev((qpos + 2) % 8), qdev((qpos + 6) % 8)
    greeted = (
        right_chip, left_chip, partner, (prev_sp, tp), (next_sp, tp),
        k_right, k_left, q_right, q_left, k_right2, k_left2, q_right2, q_left2,
    )
    for dev in greeted:
        greet(dev)
    pl.semaphore_wait(barrier, len(greeted))

    pending = []

    def send(src, dst, ssem, rsem, dev):
        cp = remote(src, dst, ssem, rsem, dev)
        cp.start()
        pending.append(cp)

    def arrived(ref, rsem):
        remote(ref, ref, rsem, rsem, partner).wait_recv()

    top, bottom = pl.ds(0, T // 2), pl.ds(T // 2, T // 2)
    halves = (top, bottom)

    def tok_send(t, half, slot, dev):
        ref = tok.at[t, halves[half], :]
        send(ref, ref, tok_s.at[slot], tok_r.at[t, half], dev)

    def tok_wait(t, half):
        arrived(tok.at[t, halves[half], :], tok_r.at[t, half])

    cp_tok.wait()
    tok_send(tp, 0, 0, right_chip)
    tok_send(tp, 1, 1, left_chip)
    tok_send(tp, 1, 2, right_chip)
    tok_send(tp, 0, 3, left_chip)
    tok_send(tp, 0, 4, partner)
    tok_send(tp, 1, 5, partner)

    for cp in loads[:9]:
        cp.wait()

    def project(t, first=False):
        block = tok[t].astype(F32)
        sq = block * block
        sq = sq[:, :128] + sq[:, 128:]
        at = pl.ds(pl.multiple_of(t * FB, FB), FB)
        scaled = (block * gain[:, at]).astype(BF)
        narrow = lax.dot_general(scaled, wn[:, at], (((1,), (1,)), ((), ())), preferred_element_type=F32)
        wide = dot(scaled, wall[at, :])
        if first:
            ss[...] = sq
            acc[:, pl.ds(0, 256)] = narrow
            acc[:, pl.ds(256, 640)] = wide
        else:
            ss[...] += sq
            acc[:, pl.ds(0, 256)] += narrow
            acc[:, pl.ds(256, 640)] += wide

    xl, xr, xo = (x + 3) % 4, (x + 1) % 4, (x + 2) % 4
    oc = 1 - c
    project(tp, True)
    tok_wait(other, 0)
    tok_wait(other, 1)
    project(other)
    tok_wait(xl * 2 + c, 0)
    tok_send(xl * 2 + c, 0, 6, right_chip)
    tok_send(xl * 2 + c, 0, 7, partner)
    tok_wait(xr * 2 + c, 1)
    tok_send(xr * 2 + c, 1, 8, left_chip)
    tok_send(xr * 2 + c, 1, 9, partner)
    tok_wait(xl * 2 + c, 1)
    tok_send(xl * 2 + c, 1, 10, partner)
    tok_wait(xr * 2 + c, 0)
    tok_send(xr * 2 + c, 0, 11, partner)
    project(xl * 2 + c)
    project(xr * 2 + c)
    tok_wait(xl * 2 + oc, 0)
    tok_wait(xl * 2 + oc, 1)
    project(xl * 2 + oc)
    tok_wait(xr * 2 + oc, 0)
    tok_wait(xr * 2 + oc, 1)
    project(xr * 2 + oc)
    tok_wait(xo * 2 + c, 0)
    tok_send(xo * 2 + c, 0, 12, partner)
    tok_wait(xo * 2 + c, 1)
    tok_send(xo * 2 + c, 1, 13, partner)
    project(xo * 2 + c)
    tok_wait(xo * 2 + oc, 0)
    tok_wait(xo * 2 + oc, 1)
    project(xo * 2 + oc)

    quarter = VD // 2

    def wa_part(t, half):
        return wa.at[pl.ds(pl.multiple_of(t * VD + half * quarter, quarter), quarter), :]

    def wa_copy(t, half, slot, dev):
        return remote(wa_part(t, half), wa_part(t, half), wa_s.at[slot], wa_r.at[t, half], dev)

    def wa_send(t, half, slot, dev):
        send(wa_part(t, half), wa_part(t, half), wa_s.at[slot], wa_r.at[t, half], dev)

    def wa_wait(t, half):
        arrived(wa_part(t, half), wa_r.at[t, half])

    for cp in loads[9:]:
        cp.wait()
    wa_send(tp, 0, 0, right_chip)
    wa_send(tp, 1, 1, left_chip)
    wa_send(tp, 1, 2, right_chip)
    wa_send(tp, 0, 3, left_chip)
    wa_send(tp, 0, 4, partner)
    wa_send(tp, 1, 5, partner)

    inv = lax.rsqrt(jnp.sum(ss[...], axis=1, keepdims=True) / D + EPS)

    def k_send(pos, slot, dev):
        send(kb.at[pos], kb.at[pos], k_s.at[slot], k_r.at[pos], dev)

    def v_send(pos, slot, dev):
        send(vb.at[pos], vb.at[pos], v_s.at[slot], v_r.at[pos], dev)

    def q_send(pos, slot, dev):
        send(qb.at[pos], qb.at[pos], q_s.at[slot], q_r.at[pos], dev)

    def q_part(pos, part, slot, dev):
        ref = qb.at[pos, pl.ds(KD * part, KD), :]
        send(ref, ref, q_s.at[slot], q_r.at[pos if part == 0 else 8], dev)

    kb[kpos] = (acc[:, 128:256] * inv).astype(BF)
    for slot, dev in enumerate((k_right2, k_left2, k_right, k_left)):
        k_send(kpos, slot, dev)
    vb[kpos] = (acc[:, 256:384] * inv).T.astype(BF)
    for slot, dev in enumerate((k_left2, k_right2, k_left, k_right)):
        v_send(kpos, slot, dev)
    qb[qpos] = (acc[:, 0:128] * (inv * QSCALE)).T.astype(BF)
    for slot, dev in enumerate((q_right2, q_left2, q_right, q_left)):
        q_send(qpos, slot, dev)

    gate[...] = (acc[:, 384:512] * inv).astype(BF)
    outer[...] = (acc[:, 512:640] * inv).astype(BF)
    pr = ((acc[:, 640:768] * inv).astype(BF).astype(F32) * (acc[:, 768:896] * inv).astype(BF).astype(F32)).astype(BF)
    pr = pr.astype(F32)
    prod[...] = pr
    edge[0] = pr[0:8]
    edge[1] = pr[T - 8 : T]
    to_prev = remote(edge.at[0], halo.at[1], h_s.at[0], h_r.at[1], (prev_sp, tp))
    to_next = remote(edge.at[1], halo.at[0], h_s.at[1], h_r.at[0], (next_sp, tp))
    to_prev.start()
    to_next.start()

    def at(pos, d):
        return (pos + d) % 8

    arrived(kb.at[at(kpos, 6)], k_r.at[at(kpos, 6)])
    k_send(at(kpos, 6), 4, k_right2)
    k_send(at(kpos, 6), 5, k_right)
    arrived(kb.at[at(kpos, 2)], k_r.at[at(kpos, 2)])
    k_send(at(kpos, 2), 6, k_left)
    arrived(vb.at[at(kpos, 2)], v_r.at[at(kpos, 2)])
    v_send(at(kpos, 2), 4, k_left2)
    v_send(at(kpos, 2), 5, k_left)
    arrived(vb.at[at(kpos, 6)], v_r.at[at(kpos, 6)])
    v_send(at(kpos, 6), 6, k_right)
    arrived(qb.at[at(qpos, 6)], q_r.at[at(qpos, 6)])
    q_part(at(qpos, 6), 0, 4, q_right2)
    q_send(at(qpos, 6), 5, q_right)
    arrived(qb.at[at(qpos, 2)], q_r.at[at(qpos, 2)])
    q_part(at(qpos, 2), 1, 6, q_left2)
    q_send(at(qpos, 2), 7, q_left)
    to_prev.wait_recv()
    to_next.wait_recv()
    before = jnp.where(sp == 0, 0.0, halo[0][7:8, :])
    after = jnp.where(sp == 63, 0.0, halo[1][0:1, :])
    cur = prod[...]
    rows = lax.broadcasted_iota(jnp.int32, (T, VD), 0)
    up = jnp.where(rows == 0, before, pltpu.roll(cur, 1, 0))
    down = jnp.where(rows == T - 1, after, pltpu.roll(cur, T - 1, 0))
    tp32 = taps[...].astype(F32)
    conv = tp32[0:1] * up + tp32[1:2] * cur + tp32[2:3] * down
    mix[c] = (outer[...].astype(F32) * conv).astype(BF)

    send(mix.at[c], mix.at[c], m_s, m_r, partner)
    send(cw_h.at[:, other_half], wout.at[c], w_s, w_r, partner)
    arrived(mix.at[1 - c], m_r)
    arrived(wout.at[1 - c], w_r)

    def p_copy(chip, core):
        return remote(
            psend.at[chip, pl.ds(pl.multiple_of(core * ROWS, ROWS), ROWS), :],
            precv.at[tp],
            p_s.at[chip * 2 + core],
            p_r.at[tp],
            (sp, chip * 2 + core),
        )

    def to_chip(i, carry):
        chip = (x + jnp.where(i == 0, 2, jnp.where(i == 1, 1, jnp.where(i == 2, 3, 0)))) % 4
        rows = pl.ds(pl.multiple_of(chip * 2 * ROWS, 2 * ROWS), 2 * ROWS)
        psend[chip] = (dot(mix[0, rows, :], wout[0]) + dot(mix[1, rows, :], wout[1])).astype(BF)

        @pl.when(i < 3)
        def _():
            p_copy(chip, c).start()

        p_copy(chip, 1 - c).start()
        return carry

    lax.fori_loop(0, 4, to_chip, 0)
    precv[tp] = psend[x, pl.ds(pl.multiple_of(c * ROWS, ROWS), ROWS), :]

    wa_wait(xl * 2 + c, 0)
    wa_send(xl * 2 + c, 0, 6, right_chip)
    wa_send(xl * 2 + c, 0, 8, partner)
    wa_wait(xr * 2 + c, 1)
    wa_send(xr * 2 + c, 1, 7, left_chip)
    wa_send(xr * 2 + c, 1, 9, partner)

    for d in (1, 7, 3, 5, 4):
        arrived(kb.at[at(kpos, d)], k_r.at[at(kpos, d)])
        arrived(vb.at[at(kpos, d)], v_r.at[at(kpos, d)])
    for d in (1, 7, 3, 5):
        arrived(qb.at[at(qpos, d)], q_r.at[at(qpos, d)])
    arrived(qb.at[at(qpos, 4), pl.ds(0, KD), :], q_r.at[at(qpos, 4)])
    arrived(qb.at[at(qpos, 4), pl.ds(KD, KD), :], q_r.at[8])

    def wa_forward():
        for slot, (t, half) in enumerate(((xl * 2 + c, 1), (xr * 2 + c, 0))):
            wa_wait(t, half)
            wa_copy(t, half, 10 + slot, partner).start()

    zero = jnp.zeros((KD, T), BF)

    def scores(qm, n, s_ref, peak):
        s = dot(kb[n], qm)
        s_ref[pl.ds(n * T, T), :] = s
        top = jnp.max(s.reshape(T // 8, 8, T), axis=0)
        return top if peak is None else jnp.maximum(peak, top)

    def apply(n, s_ref, peak, state):
        p = jnp.exp2(s_ref[pl.ds(n * T, T), :] - peak)
        part = jnp.sum(p.reshape(T // 8, 8, T), axis=0)
        o = dot(vb[n], p.astype(BF))
        return (part, o) if state is None else (state[0] + part, state[1] + o)

    def merge(a, b):
        peak = jnp.maximum(a[0], b[0])
        wa_, wb_ = jnp.exp2(a[0] - peak), jnp.exp2(b[0] - peak)
        return peak, wa_ * a[1] + wb_ * b[1], wa_ * a[2] + wb_ * b[2]

    def o_copy(pos, m):
        rows = pl.ds(m * VD, VD)
        return remote(osend.at[pos, rows, :], orecv.at[qpos, rows, :], o_s.at[pos, m], o_r.at[qpos, m], qdev(pos))

    def t_copy(pos):
        return remote(tsend.at[pos], trecv.at[qpos], st_s.at[pos], st_r.at[qpos], qdev(pos))

    def far_copies(m):
        pos = (qpos + 4) % 8
        dev = (q_right2, q_left2)[m]
        return (
            remote(osend.at[pos, pl.ds(m * VD, VD), :], rin.at[m], x_s.at[m], x_r.at[m], dev),
            remote(tsend.at[pos], rstat.at[m], x_s.at[2 + m], x_r.at[2 + m], dev),
        )

    def send_far(m):
        for cp in far_copies(m):
            cp.start()

    def send_part(i, pos, m):
        @pl.when((i == 1) | (i == 2) | (i == 5) | (i == 6))
        def _():
            o_copy(pos, m).start()
            if m == 1:
                t_copy(pos).start()

    def merge_far():
        for m in range(2):
            pos = (qpos + 2 + 4 * m) % 8
            arrived(rin.at[m], x_r.at[m])
            arrived(rstat.at[m], x_r.at[2 + m])
            rows = pl.ds(m * VD, VD)
            own, far = tsend[pos], rstat[m]
            peak, total, o = merge(
                (own[2 * m : 2 * m + 1], own[2 * m + 1 : 2 * m + 2], osend[pos, rows, :].astype(F32)),
                (far[2 * m : 2 * m + 1], far[2 * m + 1 : 2 * m + 2], rin[m].astype(F32)),
            )
            osend[pos, rows, :] = o.astype(BF)
            tsend[pos, pl.ds(2 * m, 1), :] = peak
            tsend[pos, pl.ds(2 * m + 1, 1), :] = total
            o_copy(pos, 0).start()
            o_copy(pos, 1).start()
            t_copy(pos).start()

    def ring_place(i):
        odd = i % 2
        mag = 4 - (i + 1) // 2
        return (qpos + odd * mag + (1 - odd) * ((8 - mag) % 8)) % 8

    def first_map(pos):
        return jnp.concatenate([qb[pos, pl.ds(0, KD), :], zero], axis=0)

    def second_map(pos):
        return jnp.concatenate([zero, qb[pos, pl.ds(KD, KD), :]], axis=0)

    def one_block(i, peak1):
        pos = ring_place(i)
        pl.when(i == 2)(wa_forward)
        q2 = second_map(pos)
        peak = None
        state = None
        for n in range(R):
            peak = scores(q2, n, s2, peak)
            state = apply(n, s1, peak1, state)
        peak2 = jnp.max(peak, axis=0, keepdims=True)
        sum1 = jnp.sum(state[0], axis=0, keepdims=True)
        osend[pos, pl.ds(0, VD), :] = state[1].astype(BF)
        send_part(i, pos, 0)
        q1 = first_map(ring_place((i + 1) % 8))
        peak = None
        state = None
        for n in range(R):
            peak = scores(q1, n, s1, peak)
            state = apply(n, s2, peak2, state)
        next1 = jnp.max(peak, axis=0, keepdims=True)
        sum2 = jnp.sum(state[0], axis=0, keepdims=True)
        osend[pos, pl.ds(VD, VD), :] = state[1].astype(BF)
        tsend[pos] = jnp.concatenate([peak1, sum1, peak2, sum2, peak1, sum1, peak2, sum2], axis=0)

        send_part(i, pos, 1)

        @pl.when(i == 0)
        def _():
            send_far(0)
            send_far(1)

        pl.when(i == 4)(merge_far)
        return next1

    q1 = first_map(ring_place(0))
    peak = None
    for n in range(R):
        peak = scores(q1, n, s1, peak)
    lax.fori_loop(0, 8, one_block, jnp.max(peak, axis=0, keepdims=True))

    orecv[qpos] = osend[qpos]
    trecv[qpos] = tsend[qpos]

    def part(n):
        t = trecv[n]
        return [
            (t[2 * m : 2 * m + 1], t[2 * m + 1 : 2 * m + 2], orecv[n, pl.ds(m * VD, VD), :].astype(F32))
            for m in range(2)
        ]

    def take(d, state):
        pos = (qpos + d) % 8
        for m in range(2):
            arrived(orecv.at[pos, pl.ds(m * VD, VD), :], o_r.at[pos, m])
        arrived(trecv.at[pos], st_r.at[pos])
        return [merge(a, b) for a, b in zip(state, part(pos))]

    def absorb(d):
        for m, (peak, total, o) in enumerate(take(d, [(ms[2 * m], ms[2 * m + 1], mo[m]) for m in range(2)])):
            ms[2 * m] = peak
            ms[2 * m + 1] = total
            mo[m] = o

    for m, (peak, total, o) in enumerate(part(qpos)):
        ms[2 * m] = peak
        ms[2 * m + 1] = total
        mo[m] = o
    for d in (3, 5, 1, 7, 2, 6):
        absorb(d)
    diff = mo[0] / ms[1] - lam[0] * (mo[1] / ms[3])
    diff = (diff * lax.rsqrt(jnp.mean(diff * diff, axis=0, keepdims=True) + EPS)).T
    g32 = gate[...].astype(F32)
    amix[...] = (diff * hgain[...] * (g32 / (1.0 + jnp.exp(-g32)))).astype(BF)

    mine = pl.ds(pl.multiple_of(tp * VD, VD), VD)

    def a_copy(t):
        rows = pl.ds(pl.multiple_of(t * ROWS, ROWS), ROWS)
        return remote(amix.at[rows, :], arecv.at[:, mine], a_s.at[t], a_r.at[tp], (sp, t))

    for e in (4, 5, 3, 2, 6, 1, 7):
        a_copy((tp + e) % 8).start()
    arecv[:, mine] = amix[pl.ds(pl.multiple_of(tp * ROWS, ROWS), ROWS), :]
    wa_wait(xo * 2 + c, 0)
    wa_send(xo * 2 + c, 0, 12, partner)
    wa_wait(xo * 2 + c, 1)
    wa_send(xo * 2 + c, 1, 13, partner)

    def p_wait(d, carry):
        src = (tp + d) % 8
        arrived(precv.at[src], p_r.at[src])
        return carry

    lax.fori_loop(1, 8, p_wait, 0)
    for half in range(2):
        total = precv[half].astype(F32)
        for n in range(1, 4):
            total += precv[2 * n + half].astype(F32)
        csum[:, pl.ds(half * HALF, HALF)] = total
    for t in (other, xl * 2 + oc, xr * 2 + oc, xo * 2 + oc):
        wa_wait(t, 0)
        wa_wait(t, 1)

    def add_head(t):
        cols = pl.ds(pl.multiple_of(t * VD, VD), VD)
        csum[...] += dot(arecv[:, cols], wa[cols, :])

    add_head(tp)
    for t in (other, xl * 2 + c, xl * 2 + oc, xr * 2 + c, xr * 2 + oc, xo * 2 + c, xo * 2 + oc):
        arrived(arecv.at[:, pl.ds(pl.multiple_of(t * VD, VD), VD)], a_r.at[t])
        add_head(t)
    out[...] = csum[...].astype(BF)

    for cp in pending + [*far_copies(0), *far_copies(1)]:
        cp.wait_send()
    for slot in (10, 11):
        wa_copy(tp, 0, slot, partner).wait_send()
    for d in range(1, 8):
        pos = (qpos + d) % 8
        if d != 4:
            o_copy(pos, 0).wait_send()
            o_copy(pos, 1).wait_send()
            t_copy(pos).wait_send()
        dst = (tp + d) % 8
        p_copy(dst // 2, dst % 2).wait_send()
        a_copy(dst).wait_send()
    to_prev.wait_send()
    to_next.wait_send()


def local(tokens, norm_gain, q1, k1, q2, k2, wv, wg, wo, wi, wx, taps, lam, hgain, aw, cw):
    hbm = pl.BlockSpec(memory_space=pltpu.HBM)
    vm = pl.BlockSpec(memory_space=pltpu.VMEM)
    sm = pl.BlockSpec(memory_space=pltpu.SMEM)
    dma = pltpu.SemaphoreType.DMA
    v = pltpu.VMEM
    return pl.pallas_call(
        kernel,
        out_shape=jax.ShapeDtypeStruct((ROWS, D), BF),
        in_specs=[hbm, vm] + [hbm] * 9 + [vm, sm, vm, hbm, hbm],
        out_specs=vm,
        scratch_shapes=[
            v((8, T, FB), BF), v((4 * KD, D), BF), v((D, 640), BF), v((T, 896), F32), v((T, 128), F32),
            v((R, T, 128), BF), v((R, VD, T), BF), v((R, 128, T), BF),
            v((T, VD), BF), v((T, VD), BF), v((T, VD), F32), v((2, 8, VD), F32), v((2, 8, VD), F32),
            v((KEYS, T), F32), v((KEYS, T), F32),
            v((R, 2 * VD, T), BF), v((R, 2 * VD, T), BF), v((R, 8, T), F32), v((R, 8, T), F32),
            v((2, T, VD), BF), v((2, VD, HALF), BF), v((4, 2 * ROWS, HALF), BF), v((8, ROWS, HALF), BF),
            v((8 * VD, D), BF), v((ROWS, D), F32), v((T, VD), BF), v((ROWS, 8 * VD), BF),
            v((4, 1, T), F32), v((2, VD, T), F32), v((2, VD, T), BF), v((2, 8, T), F32),
            dma((12,)), dma((14,)), dma((8, 2)), dma((8,)), dma((8,)), dma((8,)), dma((8,)), dma((8,)), dma((9,)),
            dma((8, 2)), dma((8, 2)), dma((8,)), dma((8,)), dma((2,)), dma((2,)), dma, dma, dma, dma,
            dma((8,)), dma((8,)), dma((14,)), dma((8, 2)), dma((8,)), dma((8,)), dma((4,)), dma((4,)),
        ],
        compiler_params=pltpu.CompilerParams(
            collective_id=0, has_side_effects=True, vmem_limit_bytes=56350000
        ),
        name="layer",
    )(tokens, norm_gain.reshape(1, D), q1.T, k1.T, q2.T, k2.T, wv, wg, wo, wi, wx, taps, lam, hgain.reshape(1, VD), aw, cw)


def solution(mesh):
    col = P(None, "tp")
    return jax.shard_map(
        local,
        mesh=mesh,
        in_specs=(P("sp", "tp"), P()) + (col,) * 10 + (P("tp"), P(), P("tp", None), P("tp", None)),
        out_specs=P(("sp", "tp"), None),
        check_vma=False,
    )
```

```python
import math

import jax
import jax.numpy as jnp
from jax import lax
from jax.experimental import pallas as pl
from jax.experimental.pallas import tpu as pltpu
from jax.sharding import PartitionSpec as P

MESH = pl.DeviceIdType.MESH
EPS = 1e-06
BF = jnp.bfloat16
F32 = jnp.float32
T, FB, D, R, KD, VD = 256, 256, 2048, 8, 64, 128
NTP = 8
KEYS = R * T
HALF = D // 2
ROWS = T // NTP
QSCALE = math.log2(math.e) / math.sqrt(KD)


def dot(a, b):
    return jnp.dot(a, b, preferred_element_type=F32)


def kernel(
    tok_h, gain, wq1_h, wk1_h, wq2_h, wk2_h, wv_h, wg_h, wo_h, wi_h, wx_h, taps, lam, hgain, aw_h, cw_h,
    out,
    tok, wn, wall, acc, ss, kb, vb, qb, gate, outer, prod, edge, halo, s1, s2, osend, orecv, tsend, trecv,
    mix, wout, psend, precv, wa, csum, amix, arecv, ms, mo, rin, rstat,
    lsem, tok_s, tok_r, k_s, k_r, v_s, v_r, q_s, q_r, o_s, o_r, st_s, st_r, h_s, h_r, m_s, m_r, w_s, w_r, p_s, p_r, wa_s, wa_r, a_s, a_r, x_s, x_r,
):
    sp = lax.axis_index("sp")
    tp = lax.axis_index("tp")
    c = tp % 2
    x = tp // 2
    z = sp // 8
    y = sp % 8
    kpos = (1 - c) * z + c * y
    qpos = (1 - c) * y + c * z
    kstride = 8 - 7 * c
    qstride = 1 + 7 * c
    other = x * 2 + 1 - c

    def kdev(pos):
        return (sp + (pos - kpos) * kstride, tp)

    def qdev(pos):
        return (sp + (pos - qpos) * qstride, tp)

    def remote(src, dst, ssem, rsem, dev):
        return pltpu.make_async_remote_copy(
            src_ref=src, dst_ref=dst, send_sem=ssem, recv_sem=rsem, device_id=dev, device_id_type=MESH
        )

    prev_sp = (sp + 63) % 64
    next_sp = (sp + 1) % 64

    cp_tok = pltpu.make_async_copy(tok_h, tok.at[tp], lsem.at[0])
    cp_tok.start()
    loads = []
    for i, w in enumerate((wq1_h, wq2_h, wk1_h, wk2_h)):
        loads.append(pltpu.make_async_copy(w, wn.at[pl.ds(KD * i, KD), :], lsem.at[1 + i]))
    for i, w in enumerate((wv_h, wg_h, wo_h, wi_h, wx_h)):
        loads.append(pltpu.make_async_copy(w, wall.at[:, pl.ds(128 * i, 128)], lsem.at[5 + i]))
    my_half = pl.ds(pl.multiple_of(c * HALF, HALF), HALF)
    other_half = pl.ds(pl.multiple_of((1 - c) * HALF, HALF), HALF)
    loads.append(pltpu.make_async_copy(aw_h, wa.at[pl.ds(pl.multiple_of(tp * VD, VD), VD), :], lsem.at[10]))
    loads.append(pltpu.make_async_copy(cw_h.at[:, my_half], wout.at[c], lsem.at[11]))
    for cp in loads:
        cp.start()

    barrier = pltpu.get_barrier_semaphore()

    def greet(dev):
        pl.semaphore_signal(barrier, inc=1, device_id=dev, device_id_type=MESH)

    right_chip = (sp, ((x + 1) % 4) * 2 + c)
    left_chip = (sp, ((x + 3) % 4) * 2 + c)
    partner = (sp, other)
    k_right, k_left = kdev((kpos + 1) % 8), kdev((kpos + 7) % 8)
    q_right, q_left = qdev((qpos + 1) % 8), qdev((qpos + 7) % 8)
    k_right2, k_left2 = kdev((kpos + 2) % 8), kdev((kpos + 6) % 8)
    q_right2, q_left2 = qdev((qpos + 2) % 8), qdev((qpos + 6) % 8)
    greeted = (
        right_chip, left_chip, partner, (prev_sp, tp), (next_sp, tp),
        k_right, k_left, q_right, q_left, k_right2, k_left2, q_right2, q_left2,
    )
    for dev in greeted:
        greet(dev)
    pl.semaphore_wait(barrier, len(greeted))

    pending = []

    def send(src, dst, ssem, rsem, dev):
        cp = remote(src, dst, ssem, rsem, dev)
        cp.start()
        pending.append(cp)

    def arrived(ref, rsem):
        remote(ref, ref, rsem, rsem, partner).wait_recv()

    def tok_part(t, part):
        return tok.at[t, pl.ds(part * (T // 4), T // 4), :]

    def tok_send(t, part, slot, dev):
        send(tok_part(t, part), tok_part(t, part), tok_s.at[slot], tok_r.at[t, part], dev)

    def tok_wait(t, part):
        arrived(tok_part(t, part), tok_r.at[t, part])

    def tok_block(t):
        for part in range(4):
            tok_wait(t, part)

    cp_tok.wait()
    for part in range(4):
        tok_send(tp, part, part, right_chip)
        tok_send(tp, 3 - part, 4 + part, left_chip)
    for part in range(4):
        tok_send(tp, part, 8 + part, partner)

    for cp in loads[:9]:
        cp.wait()

    def project(t, first=False):
        block = tok[t].astype(F32)
        sq = block * block
        sq = sq[:, :128] + sq[:, 128:]
        at = pl.ds(pl.multiple_of(t * FB, FB), FB)
        scaled = (block * gain[:, at]).astype(BF)
        narrow = lax.dot_general(scaled, wn[:, at], (((1,), (1,)), ((), ())), preferred_element_type=F32)
        wide = dot(scaled, wall[at, :])
        if first:
            ss[...] = sq
            acc[:, pl.ds(0, 256)] = narrow
            acc[:, pl.ds(256, 640)] = wide
        else:
            ss[...] += sq
            acc[:, pl.ds(0, 256)] += narrow
            acc[:, pl.ds(256, 640)] += wide

    xl, xr, xo = (x + 3) % 4, (x + 1) % 4, (x + 2) % 4
    oc = 1 - c
    project(tp, True)
    tok_block(other)
    project(other)
    for n in range(2):
        tok_wait(xl * 2 + c, n)
        tok_send(xl * 2 + c, n, 12 + n, right_chip)
        tok_wait(xr * 2 + c, 3 - n)
        tok_send(xr * 2 + c, 3 - n, 14 + n, left_chip)
        tok_send(xl * 2 + c, n, 16 + n, partner)
        tok_send(xr * 2 + c, 3 - n, 18 + n, partner)
    for n in range(2, 4):
        tok_wait(xl * 2 + c, n)
        tok_send(xl * 2 + c, n, 16 + n + 2, partner)
        tok_wait(xr * 2 + c, 3 - n)
        tok_send(xr * 2 + c, 3 - n, 18 + n + 2, partner)
    project(xl * 2 + c)
    project(xr * 2 + c)
    tok_block(xl * 2 + oc)
    project(xl * 2 + oc)
    tok_block(xr * 2 + oc)
    project(xr * 2 + oc)
    for slot, part in enumerate((0, 3, 1, 2)):
        tok_wait(xo * 2 + c, part)
        tok_send(xo * 2 + c, part, 24 + slot, partner)
    project(xo * 2 + c)
    tok_block(xo * 2 + oc)
    project(xo * 2 + oc)

    quarter = VD // 2

    def wa_part(t, half):
        return wa.at[pl.ds(pl.multiple_of(t * VD + half * quarter, quarter), quarter), :]

    def wa_copy(t, half, slot, dev):
        return remote(wa_part(t, half), wa_part(t, half), wa_s.at[slot], wa_r.at[t, half], dev)

    def wa_send(t, half, slot, dev):
        send(wa_part(t, half), wa_part(t, half), wa_s.at[slot], wa_r.at[t, half], dev)

    def wa_wait(t, half):
        arrived(wa_part(t, half), wa_r.at[t, half])

    for cp in loads[9:]:
        cp.wait()
    wa_send(tp, 0, 0, right_chip)
    wa_send(tp, 1, 1, left_chip)
    wa_send(tp, 1, 2, right_chip)
    wa_send(tp, 0, 3, left_chip)
    wa_send(tp, 0, 4, partner)
    wa_send(tp, 1, 5, partner)

    inv = lax.rsqrt(jnp.sum(ss[...], axis=1, keepdims=True) / D + EPS)

    def k_send(pos, slot, dev):
        send(kb.at[pos], kb.at[pos], k_s.at[slot], k_r.at[pos], dev)

    def v_send(pos, slot, dev):
        send(vb.at[pos], vb.at[pos], v_s.at[slot], v_r.at[pos], dev)

    def q_send(pos, slot, dev):
        send(qb.at[pos], qb.at[pos], q_s.at[slot], q_r.at[pos], dev)

    def q_part(pos, part, slot, dev):
        ref = qb.at[pos, pl.ds(KD * part, KD), :]
        send(ref, ref, q_s.at[slot], q_r.at[pos if part == 0 else 8], dev)

    kb[kpos] = (acc[:, 128:256] * inv).astype(BF)
    for slot, dev in enumerate((k_right2, k_left2, k_right, k_left)):
        k_send(kpos, slot, dev)
    vb[kpos] = (acc[:, 256:384] * inv).T.astype(BF)
    for slot, dev in enumerate((k_left2, k_right2, k_left, k_right)):
        v_send(kpos, slot, dev)
    qb[qpos] = (acc[:, 0:128] * (inv * QSCALE)).T.astype(BF)
    for slot, dev in enumerate((q_right2, q_left2, q_right, q_left)):
        q_send(qpos, slot, dev)

    gate[...] = (acc[:, 384:512] * inv).astype(BF)
    outer[...] = (acc[:, 512:640] * inv).astype(BF)
    pr = ((acc[:, 640:768] * inv).astype(BF).astype(F32) * (acc[:, 768:896] * inv).astype(BF).astype(F32)).astype(BF)
    pr = pr.astype(F32)
    prod[...] = pr
    edge[0] = pr[0:8]
    edge[1] = pr[T - 8 : T]
    to_prev = remote(edge.at[0], halo.at[1], h_s.at[0], h_r.at[1], (prev_sp, tp))
    to_next = remote(edge.at[1], halo.at[0], h_s.at[1], h_r.at[0], (next_sp, tp))
    to_prev.start()
    to_next.start()

    def at(pos, d):
        return (pos + d) % 8

    arrived(kb.at[at(kpos, 6)], k_r.at[at(kpos, 6)])
    k_send(at(kpos, 6), 4, k_right2)
    k_send(at(kpos, 6), 5, k_right)
    arrived(kb.at[at(kpos, 2)], k_r.at[at(kpos, 2)])
    k_send(at(kpos, 2), 6, k_left)
    arrived(qb.at[at(qpos, 6)], q_r.at[at(qpos, 6)])
    q_part(at(qpos, 6), 0, 4, q_right2)
    q_send(at(qpos, 6), 5, q_right)
    arrived(qb.at[at(qpos, 2)], q_r.at[at(qpos, 2)])
    q_part(at(qpos, 2), 1, 6, q_left2)
    q_send(at(qpos, 2), 7, q_left)
    arrived(vb.at[at(kpos, 2)], v_r.at[at(kpos, 2)])
    v_send(at(kpos, 2), 4, k_left2)
    v_send(at(kpos, 2), 5, k_left)
    arrived(vb.at[at(kpos, 6)], v_r.at[at(kpos, 6)])
    v_send(at(kpos, 6), 6, k_right)
    to_prev.wait_recv()
    to_next.wait_recv()
    before = jnp.where(sp == 0, 0.0, halo[0][7:8, :])
    after = jnp.where(sp == 63, 0.0, halo[1][0:1, :])
    cur = prod[...]
    rows = lax.broadcasted_iota(jnp.int32, (T, VD), 0)
    up = jnp.where(rows == 0, before, pltpu.roll(cur, 1, 0))
    down = jnp.where(rows == T - 1, after, pltpu.roll(cur, T - 1, 0))
    tp32 = taps[...].astype(F32)
    conv = tp32[0:1] * up + tp32[1:2] * cur + tp32[2:3] * down
    mix[c] = (outer[...].astype(F32) * conv).astype(BF)

    send(mix.at[c], mix.at[c], m_s, m_r, partner)
    send(cw_h.at[:, other_half], wout.at[c], w_s, w_r, partner)
    arrived(mix.at[1 - c], m_r)
    arrived(wout.at[1 - c], w_r)

    def p_copy(chip, core):
        return remote(
            psend.at[chip, pl.ds(pl.multiple_of(core * ROWS, ROWS), ROWS), :],
            precv.at[tp],
            p_s.at[chip * 2 + core],
            p_r.at[tp],
            (sp, chip * 2 + core),
        )

    def to_chip(i, carry):
        chip = (x + jnp.where(i == 0, 2, jnp.where(i == 1, 1, jnp.where(i == 2, 3, 0)))) % 4
        rows = pl.ds(pl.multiple_of(chip * 2 * ROWS, 2 * ROWS), 2 * ROWS)
        psend[chip] = (dot(mix[0, rows, :], wout[0]) + dot(mix[1, rows, :], wout[1])).astype(BF)

        @pl.when(i < 3)
        def _():
            p_copy(chip, c).start()

        p_copy(chip, 1 - c).start()
        return carry

    lax.fori_loop(0, 4, to_chip, 0)
    precv[tp] = psend[x, pl.ds(pl.multiple_of(c * ROWS, ROWS), ROWS), :]

    wa_wait(xl * 2 + c, 0)
    wa_send(xl * 2 + c, 0, 6, right_chip)
    wa_send(xl * 2 + c, 0, 8, partner)
    wa_wait(xr * 2 + c, 1)
    wa_send(xr * 2 + c, 1, 7, left_chip)
    wa_send(xr * 2 + c, 1, 9, partner)

    for d in (1, 7, 3, 5, 4):
        arrived(kb.at[at(kpos, d)], k_r.at[at(kpos, d)])
        arrived(vb.at[at(kpos, d)], v_r.at[at(kpos, d)])
    for d in (1, 7, 3, 5):
        arrived(qb.at[at(qpos, d)], q_r.at[at(qpos, d)])
    arrived(qb.at[at(qpos, 4), pl.ds(0, KD), :], q_r.at[at(qpos, 4)])
    arrived(qb.at[at(qpos, 4), pl.ds(KD, KD), :], q_r.at[8])

    def wa_forward():
        for slot, (t, half) in enumerate(((xl * 2 + c, 1), (xr * 2 + c, 0))):
            wa_wait(t, half)
            wa_copy(t, half, 10 + slot, partner).start()

    zero = jnp.zeros((KD, T), BF)

    def scores(qm, n, s_ref, peak):
        s = dot(kb[n], qm)
        s_ref[pl.ds(n * T, T), :] = s
        top = jnp.max(s.reshape(T // 8, 8, T), axis=0)
        return top if peak is None else jnp.maximum(peak, top)

    def apply(n, s_ref, peak, state):
        p = jnp.exp2(s_ref[pl.ds(n * T, T), :] - peak)
        part = jnp.sum(p.reshape(T // 8, 8, T), axis=0)
        o = dot(vb[n], p.astype(BF))
        return (part, o) if state is None else (state[0] + part, state[1] + o)

    def merge(a, b):
        peak = jnp.maximum(a[0], b[0])
        wa_, wb_ = jnp.exp2(a[0] - peak), jnp.exp2(b[0] - peak)
        return peak, wa_ * a[1] + wb_ * b[1], wa_ * a[2] + wb_ * b[2]

    def o_copy(pos, m):
        rows = pl.ds(m * VD, VD)
        return remote(osend.at[pos, rows, :], orecv.at[qpos, rows, :], o_s.at[pos, m], o_r.at[qpos, m], qdev(pos))

    def t_copy(pos):
        return remote(tsend.at[pos], trecv.at[qpos], st_s.at[pos], st_r.at[qpos], qdev(pos))

    def far_copies(m):
        pos = (qpos + 4) % 8
        dev = (q_right2, q_left2)[m]
        return (
            remote(osend.at[pos, pl.ds(m * VD, VD), :], rin.at[m], x_s.at[m], x_r.at[m], dev),
            remote(tsend.at[pos], rstat.at[m], x_s.at[2 + m], x_r.at[2 + m], dev),
        )

    def send_far(m):
        for cp in far_copies(m):
            cp.start()

    def send_part(i, pos, m):
        @pl.when((i == 1) | (i == 2) | (i == 5) | (i == 6))
        def _():
            o_copy(pos, m).start()
            if m == 1:
                t_copy(pos).start()

    def merge_far():
        for m in range(2):
            pos = (qpos + 2 + 4 * m) % 8
            arrived(rin.at[m], x_r.at[m])
            arrived(rstat.at[m], x_r.at[2 + m])
            rows = pl.ds(m * VD, VD)
            own, far = tsend[pos], rstat[m]
            peak, total, o = merge(
                (own[2 * m : 2 * m + 1], own[2 * m + 1 : 2 * m + 2], osend[pos, rows, :].astype(F32)),
                (far[2 * m : 2 * m + 1], far[2 * m + 1 : 2 * m + 2], rin[m].astype(F32)),
            )
            osend[pos, rows, :] = o.astype(BF)
            tsend[pos, pl.ds(2 * m, 1), :] = peak
            tsend[pos, pl.ds(2 * m + 1, 1), :] = total
            o_copy(pos, 0).start()
            o_copy(pos, 1).start()
            t_copy(pos).start()

    def ring_place(i):
        odd = i % 2
        mag = 4 - (i + 1) // 2
        return (qpos + odd * mag + (1 - odd) * ((8 - mag) % 8)) % 8

    def first_map(pos):
        return jnp.concatenate([qb[pos, pl.ds(0, KD), :], zero], axis=0)

    def second_map(pos):
        return jnp.concatenate([zero, qb[pos, pl.ds(KD, KD), :]], axis=0)

    def one_block(i, peak1):
        pos = ring_place(i)
        pl.when(i == 2)(wa_forward)
        q2 = second_map(pos)
        peak = None
        state = None
        for n in range(R):
            peak = scores(q2, n, s2, peak)
            state = apply(n, s1, peak1, state)
        peak2 = jnp.max(peak, axis=0, keepdims=True)
        sum1 = jnp.sum(state[0], axis=0, keepdims=True)
        osend[pos, pl.ds(0, VD), :] = state[1].astype(BF)
        send_part(i, pos, 0)
        q1 = first_map(ring_place((i + 1) % 8))
        peak = None
        state = None
        for n in range(R):
            peak = scores(q1, n, s1, peak)
            state = apply(n, s2, peak2, state)
        next1 = jnp.max(peak, axis=0, keepdims=True)
        sum2 = jnp.sum(state[0], axis=0, keepdims=True)
        osend[pos, pl.ds(VD, VD), :] = state[1].astype(BF)
        tsend[pos] = jnp.concatenate([peak1, sum1, peak2, sum2, peak1, sum1, peak2, sum2], axis=0)

        send_part(i, pos, 1)

        @pl.when(i == 0)
        def _():
            send_far(0)
            send_far(1)

        pl.when(i == 4)(merge_far)
        return next1

    q1 = first_map(ring_place(0))
    peak = None
    for n in range(R):
        peak = scores(q1, n, s1, peak)
    lax.fori_loop(0, 8, one_block, jnp.max(peak, axis=0, keepdims=True))

    orecv[qpos] = osend[qpos]
    trecv[qpos] = tsend[qpos]

    def part(n):
        t = trecv[n]
        return [
            (t[2 * m : 2 * m + 1], t[2 * m + 1 : 2 * m + 2], orecv[n, pl.ds(m * VD, VD), :].astype(F32))
            for m in range(2)
        ]

    def take(d, state):
        pos = (qpos + d) % 8
        for m in range(2):
            arrived(orecv.at[pos, pl.ds(m * VD, VD), :], o_r.at[pos, m])
        arrived(trecv.at[pos], st_r.at[pos])
        return [merge(a, b) for a, b in zip(state, part(pos))]

    def absorb(d):
        for m, (peak, total, o) in enumerate(take(d, [(ms[2 * m], ms[2 * m + 1], mo[m]) for m in range(2)])):
            ms[2 * m] = peak
            ms[2 * m + 1] = total
            mo[m] = o

    for m, (peak, total, o) in enumerate(part(qpos)):
        ms[2 * m] = peak
        ms[2 * m + 1] = total
        mo[m] = o
    for d in (3, 5, 1, 7, 2, 6):
        absorb(d)
    diff = mo[0] / ms[1] - lam[0] * (mo[1] / ms[3])
    diff = (diff * lax.rsqrt(jnp.mean(diff * diff, axis=0, keepdims=True) + EPS)).T
    g32 = gate[...].astype(F32)
    amix[...] = (diff * hgain[...] * (g32 / (1.0 + jnp.exp(-g32)))).astype(BF)

    mine = pl.ds(pl.multiple_of(tp * VD, VD), VD)

    def a_copy(t):
        rows = pl.ds(pl.multiple_of(t * ROWS, ROWS), ROWS)
        return remote(amix.at[rows, :], arecv.at[:, mine], a_s.at[t], a_r.at[tp], (sp, t))

    for e in (4, 5, 3, 2, 6, 1, 7):
        a_copy((tp + e) % 8).start()
    arecv[:, mine] = amix[pl.ds(pl.multiple_of(tp * ROWS, ROWS), ROWS), :]
    wa_wait(xo * 2 + c, 0)
    wa_send(xo * 2 + c, 0, 12, partner)
    wa_wait(xo * 2 + c, 1)
    wa_send(xo * 2 + c, 1, 13, partner)

    def p_wait(d, carry):
        src = (tp + d) % 8
        arrived(precv.at[src], p_r.at[src])
        return carry

    lax.fori_loop(1, 8, p_wait, 0)
    for half in range(2):
        total = precv[half].astype(F32)
        for n in range(1, 4):
            total += precv[2 * n + half].astype(F32)
        csum[:, pl.ds(half * HALF, HALF)] = total
    for t in (other, xl * 2 + oc, xr * 2 + oc, xo * 2 + oc):
        wa_wait(t, 0)
        wa_wait(t, 1)

    def add_head(t):
        cols = pl.ds(pl.multiple_of(t * VD, VD), VD)
        csum[...] += dot(arecv[:, cols], wa[cols, :])

    add_head(tp)
    for t in (other, xl * 2 + c, xl * 2 + oc, xr * 2 + c, xr * 2 + oc, xo * 2 + c, xo * 2 + oc):
        arrived(arecv.at[:, pl.ds(pl.multiple_of(t * VD, VD), VD)], a_r.at[t])
        add_head(t)
    out[...] = csum[...].astype(BF)

    for cp in pending + [*far_copies(0), *far_copies(1)]:
        cp.wait_send()
    for slot in (10, 11):
        wa_copy(tp, 0, slot, partner).wait_send()
    for d in range(1, 8):
        pos = (qpos + d) % 8
        if d != 4:
            o_copy(pos, 0).wait_send()
            o_copy(pos, 1).wait_send()
            t_copy(pos).wait_send()
        dst = (tp + d) % 8
        p_copy(dst // 2, dst % 2).wait_send()
        a_copy(dst).wait_send()
    to_prev.wait_send()
    to_next.wait_send()


def local(tokens, norm_gain, q1, k1, q2, k2, wv, wg, wo, wi, wx, taps, lam, hgain, aw, cw):
    hbm = pl.BlockSpec(memory_space=pltpu.HBM)
    vm = pl.BlockSpec(memory_space=pltpu.VMEM)
    sm = pl.BlockSpec(memory_space=pltpu.SMEM)
    dma = pltpu.SemaphoreType.DMA
    v = pltpu.VMEM
    return pl.pallas_call(
        kernel,
        out_shape=jax.ShapeDtypeStruct((ROWS, D), BF),
        in_specs=[hbm, vm] + [hbm] * 9 + [vm, sm, vm, hbm, hbm],
        out_specs=vm,
        scratch_shapes=[
            v((8, T, FB), BF), v((4 * KD, D), BF), v((D, 640), BF), v((T, 896), F32), v((T, 128), F32),
            v((R, T, 128), BF), v((R, VD, T), BF), v((R, 128, T), BF),
            v((T, VD), BF), v((T, VD), BF), v((T, VD), F32), v((2, 8, VD), F32), v((2, 8, VD), F32),
            v((KEYS, T), F32), v((KEYS, T), F32),
            v((R, 2 * VD, T), BF), v((R, 2 * VD, T), BF), v((R, 8, T), F32), v((R, 8, T), F32),
            v((2, T, VD), BF), v((2, VD, HALF), BF), v((4, 2 * ROWS, HALF), BF), v((8, ROWS, HALF), BF),
            v((8 * VD, D), BF), v((ROWS, D), F32), v((T, VD), BF), v((ROWS, 8 * VD), BF),
            v((4, 1, T), F32), v((2, VD, T), F32), v((2, VD, T), BF), v((2, 8, T), F32),
            dma((12,)), dma((28,)), dma((8, 4)), dma((8,)), dma((8,)), dma((8,)), dma((8,)), dma((8,)), dma((9,)),
            dma((8, 2)), dma((8, 2)), dma((8,)), dma((8,)), dma((2,)), dma((2,)), dma, dma, dma, dma,
            dma((8,)), dma((8,)), dma((14,)), dma((8, 2)), dma((8,)), dma((8,)), dma((4,)), dma((4,)),
        ],
        compiler_params=pltpu.CompilerParams(
            collective_id=0, has_side_effects=True, vmem_limit_bytes=56350000
        ),
        name="layer",
    )(tokens, norm_gain.reshape(1, D), q1.T, k1.T, q2.T, k2.T, wv, wg, wo, wi, wx, taps, lam, hgain.reshape(1, VD), aw, cw)


def solution(mesh):
    col = P(None, "tp")
    return jax.shard_map(
        local,
        mesh=mesh,
        in_specs=(P("sp", "tp"), P()) + (col,) * 10 + (P("tp"), P(), P("tp", None), P("tp", None)),
        out_specs=P(("sp", "tp"), None),
        check_vma=False,
    )
```

```python
import math

import jax
import jax.numpy as jnp
from jax import lax
from jax.experimental import pallas as pl
from jax.experimental.pallas import tpu as pltpu
from jax.sharding import PartitionSpec as P

MESH = pl.DeviceIdType.MESH
EPS = 1e-06
BF = jnp.bfloat16
F32 = jnp.float32
T, FB, D, R, KD, VD = 256, 256, 2048, 8, 64, 128
NTP = 8
KEYS = R * T
HALF = D // 2
ROWS = T // NTP
QSCALE = math.log2(math.e) / math.sqrt(KD)


def dot(a, b):
    return jnp.dot(a, b, preferred_element_type=F32)


def kernel(
    tok_h, gain, wq1_h, wk1_h, wq2_h, wk2_h, wv_h, wg_h, wo_h, wi_h, wx_h, taps, lam, hgain, aw_h, cw_h,
    out,
    tok, wn, wall, acc, ss, kb, vb, qb, gate, outer, prod, edge, halo, s1, s2, osend, orecv, tsend, trecv,
    mix, wout, psend, precv, wa, csum, amix, arecv, ms, mo, rin, rstat,
    lsem, tok_s, tok_r, k_s, k_r, v_s, v_r, q_s, q_r, o_s, o_r, st_s, st_r, h_s, h_r, m_s, m_r, w_s, w_r, p_s, p_r, wa_s, wa_r, a_s, a_r, x_s, x_r,
):
    sp = lax.axis_index("sp")
    tp = lax.axis_index("tp")
    c = tp % 2
    x = tp // 2
    z = sp // 8
    y = sp % 8
    kpos = (1 - c) * z + c * y
    qpos = (1 - c) * y + c * z
    kstride = 8 - 7 * c
    qstride = 1 + 7 * c
    other = x * 2 + 1 - c

    def kdev(pos):
        return (sp + (pos - kpos) * kstride, tp)

    def qdev(pos):
        return (sp + (pos - qpos) * qstride, tp)

    def remote(src, dst, ssem, rsem, dev):
        return pltpu.make_async_remote_copy(
            src_ref=src, dst_ref=dst, send_sem=ssem, recv_sem=rsem, device_id=dev, device_id_type=MESH
        )

    prev_sp = (sp + 63) % 64
    next_sp = (sp + 1) % 64

    cp_tok = pltpu.make_async_copy(tok_h, tok.at[tp], lsem.at[0])
    cp_tok.start()
    loads = []
    for i, w in enumerate((wq1_h, wq2_h, wk1_h, wk2_h)):
        loads.append(pltpu.make_async_copy(w, wn.at[pl.ds(KD * i, KD), :], lsem.at[1 + i]))
    for i, w in enumerate((wv_h, wg_h, wo_h, wi_h, wx_h)):
        loads.append(pltpu.make_async_copy(w, wall.at[:, pl.ds(128 * i, 128)], lsem.at[5 + i]))
    my_half = pl.ds(pl.multiple_of(c * HALF, HALF), HALF)
    other_half = pl.ds(pl.multiple_of((1 - c) * HALF, HALF), HALF)
    loads.append(pltpu.make_async_copy(aw_h, wa.at[pl.ds(pl.multiple_of(tp * VD, VD), VD), :], lsem.at[10]))
    loads.append(pltpu.make_async_copy(cw_h.at[:, my_half], wout.at[c], lsem.at[11]))
    for cp in loads:
        cp.start()

    barrier = pltpu.get_barrier_semaphore()

    def greet(dev):
        pl.semaphore_signal(barrier, inc=1, device_id=dev, device_id_type=MESH)

    right_chip = (sp, ((x + 1) % 4) * 2 + c)
    left_chip = (sp, ((x + 3) % 4) * 2 + c)
    partner = (sp, other)
    k_right, k_left = kdev((kpos + 1) % 8), kdev((kpos + 7) % 8)
    q_right, q_left = qdev((qpos + 1) % 8), qdev((qpos + 7) % 8)
    k_right2, k_left2 = kdev((kpos + 2) % 8), kdev((kpos + 6) % 8)
    q_right2, q_left2 = qdev((qpos + 2) % 8), qdev((qpos + 6) % 8)
    greeted = (
        right_chip, left_chip, partner, (prev_sp, tp), (next_sp, tp),
        k_right, k_left, q_right, q_left, k_right2, k_left2, q_right2, q_left2,
    )
    for dev in greeted:
        greet(dev)
    pl.semaphore_wait(barrier, len(greeted))

    pending = []

    def send(src, dst, ssem, rsem, dev):
        cp = remote(src, dst, ssem, rsem, dev)
        cp.start()
        pending.append(cp)

    def arrived(ref, rsem):
        remote(ref, ref, rsem, rsem, partner).wait_recv()

    def tok_part(t, part):
        return tok.at[t, pl.ds(part * (T // 4), T // 4), :]

    def tok_send(t, part, slot, dev):
        send(tok_part(t, part), tok_part(t, part), tok_s.at[slot], tok_r.at[t, part], dev)

    def tok_wait(t, part):
        arrived(tok_part(t, part), tok_r.at[t, part])

    def tok_block(t):
        for part in range(4):
            tok_wait(t, part)

    cp_tok.wait()
    for part in range(4):
        tok_send(tp, part, part, right_chip)
        tok_send(tp, 3 - part, 4 + part, left_chip)
    for part in range(4):
        tok_send(tp, part, 8 + part, partner)

    for cp in loads[:9]:
        cp.wait()

    def project(t, first=False):
        block = tok[t].astype(F32)
        sq = block * block
        sq = sq[:, :128] + sq[:, 128:]
        at = pl.ds(pl.multiple_of(t * FB, FB), FB)
        scaled = (block * gain[:, at]).astype(BF)
        narrow = lax.dot_general(scaled, wn[:, at], (((1,), (1,)), ((), ())), preferred_element_type=F32)
        wide = dot(scaled, wall[at, :])
        if first:
            ss[...] = sq
            acc[:, pl.ds(0, 256)] = narrow
            acc[:, pl.ds(256, 640)] = wide
        else:
            ss[...] += sq
            acc[:, pl.ds(0, 256)] += narrow
            acc[:, pl.ds(256, 640)] += wide

    xl, xr, xo = (x + 3) % 4, (x + 1) % 4, (x + 2) % 4
    oc = 1 - c
    project(tp, True)
    tok_block(other)
    project(other)
    for n in range(2):
        tok_wait(xl * 2 + c, n)
        tok_send(xl * 2 + c, n, 12 + n, right_chip)
        tok_wait(xr * 2 + c, 3 - n)
        tok_send(xr * 2 + c, 3 - n, 14 + n, left_chip)
        tok_send(xl * 2 + c, n, 16 + n, partner)
        tok_send(xr * 2 + c, 3 - n, 18 + n, partner)
    for n in range(2, 4):
        tok_wait(xl * 2 + c, n)
        tok_send(xl * 2 + c, n, 16 + n + 2, partner)
        tok_wait(xr * 2 + c, 3 - n)
        tok_send(xr * 2 + c, 3 - n, 18 + n + 2, partner)
    project(xl * 2 + c)
    project(xr * 2 + c)
    tok_block(xl * 2 + oc)
    project(xl * 2 + oc)
    tok_block(xr * 2 + oc)
    project(xr * 2 + oc)
    for slot, part in enumerate((0, 3, 1, 2)):
        tok_wait(xo * 2 + c, part)
        tok_send(xo * 2 + c, part, 24 + slot, partner)
    project(xo * 2 + c)
    tok_block(xo * 2 + oc)
    project(xo * 2 + oc)

    quarter = VD // 2

    def wa_part(t, half):
        return wa.at[pl.ds(pl.multiple_of(t * VD + half * quarter, quarter), quarter), :]

    def wa_copy(t, half, slot, dev):
        return remote(wa_part(t, half), wa_part(t, half), wa_s.at[slot], wa_r.at[t, half], dev)

    def wa_send(t, half, slot, dev):
        send(wa_part(t, half), wa_part(t, half), wa_s.at[slot], wa_r.at[t, half], dev)

    def wa_wait(t, half):
        arrived(wa_part(t, half), wa_r.at[t, half])

    for cp in loads[9:]:
        cp.wait()
    wa_send(tp, 0, 0, right_chip)
    wa_send(tp, 1, 1, left_chip)
    wa_send(tp, 1, 2, right_chip)
    wa_send(tp, 0, 3, left_chip)
    wa_send(tp, 0, 4, partner)
    wa_send(tp, 1, 5, partner)

    inv = lax.rsqrt(jnp.sum(ss[...], axis=1, keepdims=True) / D + EPS)

    def k_send(pos, slot, dev):
        send(kb.at[pos], kb.at[pos], k_s.at[slot], k_r.at[pos], dev)

    def v_send(pos, slot, dev):
        send(vb.at[pos], vb.at[pos], v_s.at[slot], v_r.at[pos], dev)

    def q_send(pos, slot, dev):
        send(qb.at[pos], qb.at[pos], q_s.at[slot], q_r.at[pos], dev)

    def q_part(pos, part, slot, dev):
        ref = qb.at[pos, pl.ds(KD * part, KD), :]
        send(ref, ref, q_s.at[slot], q_r.at[pos if part == 0 else 8], dev)

    kb[kpos] = (acc[:, 128:256] * inv).astype(BF)
    for slot, dev in enumerate((k_right2, k_left2, k_right, k_left)):
        k_send(kpos, slot, dev)
    vb[kpos] = (acc[:, 256:384] * inv).T.astype(BF)
    for slot, dev in enumerate((k_left2, k_right2, k_left, k_right)):
        v_send(kpos, slot, dev)
    qb[qpos] = (acc[:, 0:128] * (inv * QSCALE)).T.astype(BF)
    for slot, dev in enumerate((q_right2, q_left2, q_right, q_left)):
        q_send(qpos, slot, dev)

    gate[...] = (acc[:, 384:512] * inv).astype(BF)
    outer[...] = (acc[:, 512:640] * inv).astype(BF)
    pr = ((acc[:, 640:768] * inv).astype(BF).astype(F32) * (acc[:, 768:896] * inv).astype(BF).astype(F32)).astype(BF)
    pr = pr.astype(F32)
    prod[...] = pr
    edge[0] = pr[0:8]
    edge[1] = pr[T - 8 : T]
    to_prev = remote(edge.at[0], halo.at[1], h_s.at[0], h_r.at[1], (prev_sp, tp))
    to_next = remote(edge.at[1], halo.at[0], h_s.at[1], h_r.at[0], (next_sp, tp))
    to_prev.start()
    to_next.start()

    def at(pos, d):
        return (pos + d) % 8

    arrived(kb.at[at(kpos, 6)], k_r.at[at(kpos, 6)])
    k_send(at(kpos, 6), 4, k_right2)
    k_send(at(kpos, 6), 5, k_right)
    arrived(kb.at[at(kpos, 2)], k_r.at[at(kpos, 2)])
    k_send(at(kpos, 2), 6, k_left)
    arrived(qb.at[at(qpos, 6)], q_r.at[at(qpos, 6)])
    q_part(at(qpos, 6), 0, 4, q_right2)
    q_send(at(qpos, 6), 5, q_right)
    arrived(qb.at[at(qpos, 2)], q_r.at[at(qpos, 2)])
    q_part(at(qpos, 2), 1, 6, q_left2)
    q_send(at(qpos, 2), 7, q_left)
    arrived(vb.at[at(kpos, 2)], v_r.at[at(kpos, 2)])
    v_send(at(kpos, 2), 4, k_left2)
    v_send(at(kpos, 2), 5, k_left)
    arrived(vb.at[at(kpos, 6)], v_r.at[at(kpos, 6)])
    v_send(at(kpos, 6), 6, k_right)
    to_prev.wait_recv()
    to_next.wait_recv()
    before = jnp.where(sp == 0, 0.0, halo[0][7:8, :])
    after = jnp.where(sp == 63, 0.0, halo[1][0:1, :])
    cur = prod[...]
    rows = lax.broadcasted_iota(jnp.int32, (T, VD), 0)
    up = jnp.where(rows == 0, before, pltpu.roll(cur, 1, 0))
    down = jnp.where(rows == T - 1, after, pltpu.roll(cur, T - 1, 0))
    tp32 = taps[...].astype(F32)
    conv = tp32[0:1] * up + tp32[1:2] * cur + tp32[2:3] * down
    mix[c] = (outer[...].astype(F32) * conv).astype(BF)

    send(mix.at[c], mix.at[c], m_s, m_r, partner)
    send(cw_h.at[:, other_half], wout.at[c], w_s, w_r, partner)
    arrived(mix.at[1 - c], m_r)
    arrived(wout.at[1 - c], w_r)

    def p_copy(chip, core):
        return remote(
            psend.at[chip, pl.ds(pl.multiple_of(core * ROWS, ROWS), ROWS), :],
            precv.at[tp],
            p_s.at[chip * 2 + core],
            p_r.at[tp],
            (sp, chip * 2 + core),
        )

    def to_chip(i, carry):
        chip = (x + jnp.where(i == 0, 2, jnp.where(i == 1, 1, jnp.where(i == 2, 3, 0)))) % 4
        rows = pl.ds(pl.multiple_of(chip * 2 * ROWS, 2 * ROWS), 2 * ROWS)
        psend[chip] = (dot(mix[0, rows, :], wout[0]) + dot(mix[1, rows, :], wout[1])).astype(BF)

        @pl.when(i < 3)
        def _():
            p_copy(chip, c).start()

        p_copy(chip, 1 - c).start()
        return carry

    lax.fori_loop(0, 4, to_chip, 0)
    precv[tp] = psend[x, pl.ds(pl.multiple_of(c * ROWS, ROWS), ROWS), :]

    wa_wait(xl * 2 + c, 0)
    wa_send(xl * 2 + c, 0, 6, right_chip)
    wa_send(xl * 2 + c, 0, 8, partner)
    wa_wait(xr * 2 + c, 1)
    wa_send(xr * 2 + c, 1, 7, left_chip)
    wa_send(xr * 2 + c, 1, 9, partner)

    for d in (1, 7, 3, 5, 4):
        arrived(kb.at[at(kpos, d)], k_r.at[at(kpos, d)])
        arrived(vb.at[at(kpos, d)], v_r.at[at(kpos, d)])
    for d in (1, 7, 3, 5):
        arrived(qb.at[at(qpos, d)], q_r.at[at(qpos, d)])
    arrived(qb.at[at(qpos, 4), pl.ds(0, KD), :], q_r.at[at(qpos, 4)])
    arrived(qb.at[at(qpos, 4), pl.ds(KD, KD), :], q_r.at[8])

    def wa_forward():
        for slot, (t, half) in enumerate(((xl * 2 + c, 1), (xr * 2 + c, 0))):
            wa_wait(t, half)
            wa_copy(t, half, 10 + slot, partner).start()

    zero = jnp.zeros((KD, T), BF)

    def scores(qm, n, s_ref, peak):
        s = dot(kb[n], qm)
        s_ref[pl.ds(n * T, T), :] = s
        top = jnp.max(s.reshape(T // 8, 8, T), axis=0)
        return top if peak is None else jnp.maximum(peak, top)

    def apply(n, s_ref, peak, state):
        p = jnp.exp2(s_ref[pl.ds(n * T, T), :] - peak)
        part = jnp.sum(p.reshape(T // 8, 8, T), axis=0)
        o = dot(vb[n], p.astype(BF))
        return (part, o) if state is None else (state[0] + part, state[1] + o)

    def merge(a, b):
        peak = jnp.maximum(a[0], b[0])
        wa_, wb_ = jnp.exp2(a[0] - peak), jnp.exp2(b[0] - peak)
        return peak, wa_ * a[1] + wb_ * b[1], wa_ * a[2] + wb_ * b[2]

    def o_copy(pos, m):
        rows = pl.ds(m * VD, VD)
        return remote(osend.at[pos, rows, :], orecv.at[qpos, rows, :], o_s.at[pos, m], o_r.at[qpos, m], qdev(pos))

    def t_copy(pos):
        return remote(tsend.at[pos], trecv.at[qpos], st_s.at[pos], st_r.at[qpos], qdev(pos))

    def far_copies(m):
        pos = (qpos + 4) % 8
        dev = (q_right2, q_left2)[m]
        return (
            remote(osend.at[pos, pl.ds(m * VD, VD), :], rin.at[m], x_s.at[m], x_r.at[m], dev),
            remote(tsend.at[pos], rstat.at[m], x_s.at[2 + m], x_r.at[2 + m], dev),
        )

    def send_far(m):
        for cp in far_copies(m):
            cp.start()

    def send_part(i, pos, m):
        @pl.when((i == 1) | (i == 2) | (i == 5) | (i == 6))
        def _():
            o_copy(pos, m).start()
            if m == 1:
                t_copy(pos).start()

    def merge_far():
        for m in range(2):
            pos = (qpos + 2 + 4 * m) % 8
            arrived(rin.at[m], x_r.at[m])
            arrived(rstat.at[m], x_r.at[2 + m])
            rows = pl.ds(m * VD, VD)
            own, far = tsend[pos], rstat[m]
            peak, total, o = merge(
                (own[2 * m : 2 * m + 1], own[2 * m + 1 : 2 * m + 2], osend[pos, rows, :].astype(F32)),
                (far[2 * m : 2 * m + 1], far[2 * m + 1 : 2 * m + 2], rin[m].astype(F32)),
            )
            osend[pos, rows, :] = o.astype(BF)
            tsend[pos, pl.ds(2 * m, 1), :] = peak
            tsend[pos, pl.ds(2 * m + 1, 1), :] = total
            o_copy(pos, 0).start()
            o_copy(pos, 1).start()
            t_copy(pos).start()

    def ring_place(i):
        odd = i % 2
        mag = 4 - (i + 1) // 2
        return (qpos + odd * mag + (1 - odd) * ((8 - mag) % 8)) % 8

    def first_map(pos):
        return jnp.concatenate([qb[pos, pl.ds(0, KD), :], zero], axis=0)

    def second_map(pos):
        return jnp.concatenate([zero, qb[pos, pl.ds(KD, KD), :]], axis=0)

    def one_block(i, peak1, last=False):
        pos = ring_place(i)
        pl.when(i == 2)(wa_forward)
        q2 = second_map(pos)
        peak = None
        state = None
        for n in range(R):
            peak = scores(q2, n, s2, peak)
            state = apply(n, s1, peak1, state)
        peak2 = jnp.max(peak, axis=0, keepdims=True)
        sum1 = jnp.sum(state[0], axis=0, keepdims=True)
        osend[pos, pl.ds(0, VD), :] = state[1].astype(BF)
        send_part(i, pos, 0)
        q1 = None if last else first_map(ring_place((i + 1) % 8))
        peak = None
        state = None
        for n in range(R):
            if not last:
                peak = scores(q1, n, s1, peak)
            state = apply(n, s2, peak2, state)
        next1 = peak1 if last else jnp.max(peak, axis=0, keepdims=True)
        sum2 = jnp.sum(state[0], axis=0, keepdims=True)
        osend[pos, pl.ds(VD, VD), :] = state[1].astype(BF)
        tsend[pos] = jnp.concatenate([peak1, sum1, peak2, sum2, peak1, sum1, peak2, sum2], axis=0)

        send_part(i, pos, 1)

        @pl.when(i == 0)
        def _():
            send_far(0)
            send_far(1)

        pl.when(i == 4)(merge_far)
        return next1

    q1 = first_map(ring_place(0))
    peak = None
    for n in range(R):
        peak = scores(q1, n, s1, peak)
    peak = lax.fori_loop(0, 7, one_block, jnp.max(peak, axis=0, keepdims=True))
    one_block(7, peak, last=True)

    orecv[qpos] = osend[qpos]
    trecv[qpos] = tsend[qpos]

    def part(n):
        t = trecv[n]
        return [
            (t[2 * m : 2 * m + 1], t[2 * m + 1 : 2 * m + 2], orecv[n, pl.ds(m * VD, VD), :].astype(F32))
            for m in range(2)
        ]

    def take(d, state):
        pos = (qpos + d) % 8
        for m in range(2):
            arrived(orecv.at[pos, pl.ds(m * VD, VD), :], o_r.at[pos, m])
        arrived(trecv.at[pos], st_r.at[pos])
        return [merge(a, b) for a, b in zip(state, part(pos))]

    def absorb(d):
        for m, (peak, total, o) in enumerate(take(d, [(ms[2 * m], ms[2 * m + 1], mo[m]) for m in range(2)])):
            ms[2 * m] = peak
            ms[2 * m + 1] = total
            mo[m] = o

    for m, (peak, total, o) in enumerate(part(qpos)):
        ms[2 * m] = peak
        ms[2 * m + 1] = total
        mo[m] = o
    for d in (3, 5, 1, 7, 2, 6):
        absorb(d)
    diff = mo[0] / ms[1] - lam[0] * (mo[1] / ms[3])
    diff = (diff * lax.rsqrt(jnp.mean(diff * diff, axis=0, keepdims=True) + EPS)).T
    g32 = gate[...].astype(F32)
    amix[...] = (diff * hgain[...] * (g32 / (1.0 + jnp.exp(-g32)))).astype(BF)

    mine = pl.ds(pl.multiple_of(tp * VD, VD), VD)

    def a_copy(t):
        rows = pl.ds(pl.multiple_of(t * ROWS, ROWS), ROWS)
        return remote(amix.at[rows, :], arecv.at[:, mine], a_s.at[t], a_r.at[tp], (sp, t))

    for e in (4, 5, 3, 2, 6, 1, 7):
        a_copy((tp + e) % 8).start()
    arecv[:, mine] = amix[pl.ds(pl.multiple_of(tp * ROWS, ROWS), ROWS), :]
    wa_wait(xo * 2 + c, 0)
    wa_send(xo * 2 + c, 0, 12, partner)
    wa_wait(xo * 2 + c, 1)
    wa_send(xo * 2 + c, 1, 13, partner)

    def p_wait(d, carry):
        src = (tp + d) % 8
        arrived(precv.at[src], p_r.at[src])
        return carry

    lax.fori_loop(1, 8, p_wait, 0)
    for half in range(2):
        total = precv[half].astype(F32)
        for n in range(1, 4):
            total += precv[2 * n + half].astype(F32)
        csum[:, pl.ds(half * HALF, HALF)] = total
    for t in (other, xl * 2 + oc, xr * 2 + oc, xo * 2 + oc):
        wa_wait(t, 0)
        wa_wait(t, 1)

    def add_head(t):
        cols = pl.ds(pl.multiple_of(t * VD, VD), VD)
        csum[...] += dot(arecv[:, cols], wa[cols, :])

    add_head(tp)
    for t in (other, xl * 2 + c, xl * 2 + oc, xr * 2 + c, xr * 2 + oc, xo * 2 + c, xo * 2 + oc):
        arrived(arecv.at[:, pl.ds(pl.multiple_of(t * VD, VD), VD)], a_r.at[t])
        add_head(t)
    out[...] = csum[...].astype(BF)

    for cp in pending + [*far_copies(0), *far_copies(1)]:
        cp.wait_send()
    for slot in (10, 11):
        wa_copy(tp, 0, slot, partner).wait_send()
    for d in range(1, 8):
        pos = (qpos + d) % 8
        if d != 4:
            o_copy(pos, 0).wait_send()
            o_copy(pos, 1).wait_send()
            t_copy(pos).wait_send()
        dst = (tp + d) % 8
        p_copy(dst // 2, dst % 2).wait_send()
        a_copy(dst).wait_send()
    to_prev.wait_send()
    to_next.wait_send()


def local(tokens, norm_gain, q1, k1, q2, k2, wv, wg, wo, wi, wx, taps, lam, hgain, aw, cw):
    hbm = pl.BlockSpec(memory_space=pltpu.HBM)
    vm = pl.BlockSpec(memory_space=pltpu.VMEM)
    sm = pl.BlockSpec(memory_space=pltpu.SMEM)
    dma = pltpu.SemaphoreType.DMA
    v = pltpu.VMEM
    return pl.pallas_call(
        kernel,
        out_shape=jax.ShapeDtypeStruct((ROWS, D), BF),
        in_specs=[hbm, vm] + [hbm] * 9 + [vm, sm, vm, hbm, hbm],
        out_specs=vm,
        scratch_shapes=[
            v((8, T, FB), BF), v((4 * KD, D), BF), v((D, 640), BF), v((T, 896), F32), v((T, 128), F32),
            v((R, T, 128), BF), v((R, VD, T), BF), v((R, 128, T), BF),
            v((T, VD), BF), v((T, VD), BF), v((T, VD), F32), v((2, 8, VD), F32), v((2, 8, VD), F32),
            v((KEYS, T), F32), v((KEYS, T), F32),
            v((R, 2 * VD, T), BF), v((R, 2 * VD, T), BF), v((R, 8, T), F32), v((R, 8, T), F32),
            v((2, T, VD), BF), v((2, VD, HALF), BF), v((4, 2 * ROWS, HALF), BF), v((8, ROWS, HALF), BF),
            v((8 * VD, D), BF), v((ROWS, D), F32), v((T, VD), BF), v((ROWS, 8 * VD), BF),
            v((4, 1, T), F32), v((2, VD, T), F32), v((2, VD, T), BF), v((2, 8, T), F32),
            dma((12,)), dma((28,)), dma((8, 4)), dma((8,)), dma((8,)), dma((8,)), dma((8,)), dma((8,)), dma((9,)),
            dma((8, 2)), dma((8, 2)), dma((8,)), dma((8,)), dma((2,)), dma((2,)), dma, dma, dma, dma,
            dma((8,)), dma((8,)), dma((14,)), dma((8, 2)), dma((8,)), dma((8,)), dma((4,)), dma((4,)),
        ],
        compiler_params=pltpu.CompilerParams(
            collective_id=0, has_side_effects=True, vmem_limit_bytes=56350000
        ),
        name="layer",
    )(tokens, norm_gain.reshape(1, D), q1.T, k1.T, q2.T, k2.T, wv, wg, wo, wi, wx, taps, lam, hgain.reshape(1, VD), aw, cw)


def solution(mesh):
    col = P(None, "tp")
    return jax.shard_map(
        local,
        mesh=mesh,
        in_specs=(P("sp", "tp"), P()) + (col,) * 10 + (P("tp"), P(), P("tp", None), P("tp", None)),
        out_specs=P(("sp", "tp"), None),
        check_vma=False,
    )
```
